512 devices in a mesh: grp: 2 (over y), fs: 32 (over z), tp: 8 (over x, core).
Axes of the slice: x: 4, y: 2, z: 32, core: 2. Of those that a mesh axis runs over, the one named last changes fastest.
The devices are a block of a 4x8x32 slice.
Arguments:
- tokens: bfloat16 [64, 384, 2048], P(('grp', 'fs'), None, 'tp'), parts along dimension 0, may hold values from -24 to 24
- input_gain: float32 [2048], replicated, may hold values from 0.1 to 1.9
- query_weight: bfloat16 [2048, 1024], P('fs', 'tp'), may hold values from -0.125 to 0.125
- key_weight: bfloat16 [2048, 1024], P('fs', 'tp'), may hold values from -0.125 to 0.125
- value_weight: bfloat16 [2048, 1024], P('fs', 'tp'), may hold values from -0.125 to 0.125
- output_gate_matrix: bfloat16 [2048, 1024], P('fs', 'tp'), may hold values from -0.125 to 0.125
- forward_decay: float32 [16], P('tp'), may hold values from -1 to 9
- backward_decay: float32 [16], P('tp'), may hold values from -1 to 9
- merge_weight: bfloat16 [1024, 2048], P('tp', 'fs'), may hold values from -0.375 to 0.375
- middle_gain: float32 [2048], replicated, may hold values from 0.1 to 1.9
- gate_weight: bfloat16 [2048, 5120], P('fs', 'tp'), may hold values from -0.125 to 0.125
- up_weight: bfloat16 [2048, 5120], P('fs', 'tp'), may hold values from -0.125 to 0.125
- down_weight: bfloat16 [5120, 2048], P('tp', 'fs'), may hold values from -0.15625 to 0.15625
Outputs:
- layer_out: bfloat16 [64, 384, 2048], P(('grp', 'fs'), None, 'tp'), parts along dimension 0
The draws below stay inside these ranges and needn't reach their ends.
There are 2 independent parts, one for each index of `grp`. The reference program is written for one: setup_inputs(seed, part) draws one part's arguments, and reference() takes and returns one part's arrays. A program takes and returns all parts, laid end to end along the dimension named above; an argument that names none is the same for every part. Nothing has to cross between parts.
All inputs are finite; a program needn't handle non-finite values.
Results may differ from the reference program's by a relative error of at most 0.019.
Values may be sent and summed in bfloat16 or wider, within the bound.
No kernel may reach another device: no remote copies, remote signals or barrier semaphores. Data moves between devices by JAX's collectives and lax.ppermute only.
A program may use at most 64 MiB of HBM per device.

```python
import math
import jax
import jax.numpy as jnp
from jax import lax

D = 2048
HEADS = 16
FF = 5120
BLOCK = 128
LEN = 384
RET_W = 1024
SEQS = 32
N_TP = 8


def draw_tokens(key, part):
    subkeys = jax.random.split(jax.random.fold_in(key, 11), 3)
    full_shape = (SEQS, LEN, D)
    row_scale = jnp.exp(jax.random.uniform(subkeys[1], (SEQS, LEN, 1), jnp.float32, math.log(0.3), math.log(3.0)))
    column_scale = jnp.exp(jax.random.uniform(subkeys[2], (1, 1, D), jnp.float32, math.log(0.5), math.log(2.0)))
    base_values = jnp.clip(jax.random.normal(subkeys[0], full_shape, jnp.float32), -4.0, 4.0)
    return (base_values * row_scale * column_scale).astype(jnp.bfloat16)


def decay_logits(key, salt):
    subkeys = jax.random.split(jax.random.fold_in(key, salt), 3)
    slow_share = 0.5
    slow_low = 0.7
    slow_high = 2.3
    is_slow = jax.random.bernoulli(subkeys[0], slow_share, (HEADS,))
    slow_rate = -jax.random.uniform(subkeys[1], (HEADS,), jnp.float32, slow_low, slow_high) / LEN
    fast_rate = -jax.random.uniform(subkeys[2], (HEADS,), jnp.float32, 7.5, 15.0) / BLOCK
    log_rates = jnp.where(is_slow, slow_rate, fast_rate)
    return log_rates - jnp.log(-jnp.expm1(log_rates))


def draw_forward_decay(key, part):
    return decay_logits(key, 21)


def draw_backward_decay(key, part):
    return decay_logits(key, 22)


def levels(stream_key, dims, pieces, smallest, largest):
    gain, own = 1.0, jax.random.fold_in(stream_key, 6)
    for dim, blocks in pieces:
        draws = jnp.exp(jax.random.uniform(jax.random.fold_in(own, dim), (blocks,), jnp.float32, smallest / len(pieces), largest / len(pieces)))
        gain = gain * jnp.repeat(draws, dims[dim] // blocks).reshape([-1 if axis == dim else 1 for axis in range(len(dims))])
    return gain


def scatter_about(stream_key, shape, scale, bound, cuts=(), kind=jnp.bfloat16):
    level = levels(stream_key, shape, cuts, -0.22, 0.18) if cuts else 1.0
    values = jax.random.normal(stream_key, shape, jnp.float32) * scale * level
    return jnp.minimum(jnp.maximum(values, -bound), bound).astype(kind)


def setup_inputs(seed: int = 0, part: int = 0) -> dict:
    arg_keys = jax.random.split(jax.random.key(seed), 14)
    part_splits = jax.random.split(jax.random.fold_in(arg_keys[13], part), 14)
    return {
        "tokens": draw_tokens(jax.random.fold_in(jax.random.fold_in(arg_keys[13], part), 71), part),
        "input_gain": jnp.clip(1.0 + 0.18 * jax.random.normal(arg_keys[1], (D,), jnp.float32), 0.1, 1.9),
        "query_weight": scatter_about(arg_keys[2], (D, RET_W), D ** -0.5, 0.125, ((0, 32), (1, 8))),
        "key_weight": scatter_about(arg_keys[3], (D, RET_W), D ** -0.5, 0.125, ((0, 32), (1, 8))),
        "value_weight": scatter_about(arg_keys[4], (D, RET_W), D ** -0.5, 0.125, ((0, 32), (1, 8))),
        "output_gate_matrix": scatter_about(arg_keys[5], (D, RET_W), D ** -0.5, 0.125, ((0, 32), (1, 8))),
        "forward_decay": draw_forward_decay(jax.random.fold_in(arg_keys[13], 71), part),
        "backward_decay": draw_backward_decay(jax.random.fold_in(arg_keys[13], 71), part),
        "merge_weight": scatter_about(arg_keys[8], (RET_W, D), (RET_W // 4) ** -0.5, 0.375, ((0, 8), (1, 32))),
        "middle_gain": jnp.clip(1.0 + 0.18 * jax.random.normal(arg_keys[9], (D,), jnp.float32), 0.1, 1.9),
        "gate_weight": scatter_about(arg_keys[10], (D, FF), D ** -0.5, 0.125, ((0, 32), (1, 8))),
        "up_weight": scatter_about(arg_keys[11], (D, FF), D ** -0.5, 0.125, ((0, 32), (1, 8))),
        "down_weight": scatter_about(arg_keys[12], (FF, D), (FF // 4) ** -0.5, 0.15625, ((0, 8), (1, 32))),
    }


norm_eps = 1e-06
group_eps = 1e-05
rope_base = 10000.0
highest_precision = lax.Precision.HIGHEST

def rms_scale(values, gain_vector):
    widened = values.astype(jnp.float32)
    scaled = widened * lax.rsqrt(lax.optimization_barrier(jnp.mean(widened * widened, axis=-1, keepdims=True)) + norm_eps)
    return (scaled * gain_vector.astype(jnp.float32)).astype(jnp.bfloat16)

def apply_rotary_heads(values, length):
    half_dim = values.shape[-1] // 2
    inverse = rope_base ** (-jnp.arange(half_dim, dtype=jnp.float32) / half_dim)
    angles = jnp.arange(length, dtype=jnp.float32)[:, None] * inverse[None, :]
    cosine = jnp.cos(angles)[:, None, :]
    sine_part = jnp.sin(angles)[:, None, :]
    lower_half = values[..., :half_dim]
    upper_half = values[..., half_dim:]
    return jnp.concatenate([lower_half * cosine - upper_half * sine_part, upper_half * cosine + lower_half * sine_part], axis=-1)

def retain_dense(query_rows, key_rows, value_rows, gate_rows, forward_decay, backward_decay, seq_count, length):
    head_count = forward_decay.shape[0]
    head_dim = query_rows.shape[1] // head_count

    def split_heads(rows_in):
        return rows_in.astype(jnp.float32).reshape(seq_count, length, head_count, head_dim)
    queries = apply_rotary_heads(split_heads(query_rows), length)
    key_heads = apply_rotary_heads(split_heads(key_rows), length) * head_dim ** (-0.5)
    valued = split_heads(value_rows)
    rate_ahead = jax.nn.log_sigmoid(forward_decay.astype(jnp.float32))
    rate_behind = jax.nn.log_sigmoid(backward_decay.astype(jnp.float32))
    position = jnp.arange(length, dtype=jnp.float32)
    offset = position[:, None] - position[None, :]
    weight_tree = jnp.where(offset[None] >= 0, jnp.exp(rate_ahead[:, None, None] * jnp.maximum(offset, 0.0)[None]), jnp.exp(rate_behind[:, None, None] * jnp.maximum(-offset, 0.0)[None]))

    def one_sequence(operands):
        sequence_query, sequence_key, sequence_value = operands
        attention_scores = jnp.einsum('pze,rze->zpr', sequence_query, sequence_key, precision=highest_precision) * weight_tree
        return jnp.einsum('kaf,fkg->akg', attention_scores, sequence_value, precision=highest_precision)
    result = lax.map(one_sequence, (queries, key_heads, valued))
    center = lax.optimization_barrier(jnp.mean(result, axis=-1, keepdims=True))
    spread = lax.optimization_barrier(jnp.mean(jnp.square(result - center), axis=-1, keepdims=True))
    normalized = (result - center) * lax.rsqrt(spread + group_eps)
    gated = jax.nn.silu(split_heads(gate_rows)) * normalized
    return gated.reshape(seq_count * length, head_count * head_dim).astype(jnp.bfloat16)

def split_sum(left_rows, right_rows):
    group_size = left_rows.shape[1] // N_TP
    total = jnp.zeros((left_rows.shape[0], right_rows.shape[1]), jnp.float32)
    for index in range(N_TP):
        lower = index * group_size
        partial_term = jnp.dot(left_rows[:, lower:lower + group_size], right_rows[lower:lower + group_size], preferred_element_type=jnp.float32).astype(jnp.bfloat16)
        total = total + lax.optimization_barrier(partial_term).astype(jnp.float32)
    return total

def reference(tokens, input_gain, query_weight, key_weight, value_weight, output_gate_matrix, forward_decay, backward_decay, merge_weight, middle_gain, gate_weight, up_weight, down_weight):
    seq_count, length, width = tokens.shape
    row_count = seq_count * length
    flat = tokens.reshape(row_count, width)
    normed = rms_scale(flat, input_gain)
    query_rows = jnp.dot(normed, query_weight, preferred_element_type=jnp.float32).astype(jnp.bfloat16)
    key_rows = jnp.dot(normed, key_weight, preferred_element_type=jnp.float32).astype(jnp.bfloat16)
    value_rows = jnp.dot(normed, value_weight, preferred_element_type=jnp.float32).astype(jnp.bfloat16)
    gate_rows = jnp.dot(normed, output_gate_matrix, preferred_element_type=jnp.float32).astype(jnp.bfloat16)
    mixed = retain_dense(query_rows, key_rows, value_rows, gate_rows, forward_decay, backward_decay, seq_count, length)
    middle = (flat.astype(jnp.float32) + split_sum(mixed, merge_weight)).astype(jnp.bfloat16)
    normed_mid = rms_scale(middle, middle_gain)
    gate_act = jnp.dot(normed_mid, gate_weight, preferred_element_type=jnp.float32)
    up_act = jnp.dot(normed_mid, up_weight, preferred_element_type=jnp.float32)
    hidden = (jax.nn.silu(gate_act) * up_act).astype(jnp.bfloat16)
    layer_out = (middle.astype(jnp.float32) + split_sum(hidden, down_weight)).astype(jnp.bfloat16)
    return layer_out.reshape(seq_count, length, width)
```

```python
import jax
import jax.numpy as jnp
from jax import lax
from jax.sharding import PartitionSpec as P

BLOCK = 128


norm_eps = 1e-06
group_eps = 1e-05
rope_base = 10000.0
highest_precision = lax.Precision.HIGHEST


def core_pairs():
    peers = lax.axis_size("tp")
    return [[i, i + 1] for i in range(0, peers, 2)]


def chip_rings():
    peers = lax.axis_size("tp")
    return [list(range(0, peers, 2)), list(range(1, peers, 2))]


def gathered_features(shard):
    chips = lax.all_gather(shard, "tp", axis=0, axis_index_groups=chip_rings())
    both = jnp.broadcast_to(chips, (2, *chips.shape))
    both = lax.all_to_all(both, "tp", 0, 0, tiled=True, axis_index_groups=core_pairs())
    return jnp.concatenate(
        [both[c, x] for x in range(chips.shape[0]) for c in range(2)], axis=1
    )


def scattered_sum(partial_term):
    peers = lax.axis_size("tp")
    rows, width = partial_term.shape[0], partial_term.shape[1] // peers
    parts = [partial_term[:, t * width : (t + 1) * width] for t in range(peers)]
    tiles = jnp.stack([jnp.stack(parts[0::2]), jnp.stack(parts[1::2])])
    tiles = lax.all_to_all(tiles, "tp", 0, 0, tiled=True, axis_index_groups=core_pairs())
    chip_sum = (tiles[0].astype(jnp.float32) + tiles[1].astype(jnp.float32)).astype(jnp.bfloat16)
    tiles = lax.all_to_all(chip_sum, "tp", 0, 0, tiled=True, axis_index_groups=chip_rings())
    return jnp.sum(tiles.astype(jnp.float32), axis=0)


def rms_scale(values, gain_vector):
    widened = values.astype(jnp.float32)
    scaled = widened * lax.rsqrt(jnp.mean(widened * widened, axis=-1, keepdims=True) + norm_eps)
    return (scaled * gain_vector).astype(jnp.bfloat16)


def apply_rotary_heads(values, length):
    half_dim = values.shape[-1] // 2
    inverse = rope_base ** (-jnp.arange(half_dim, dtype=jnp.float32) / half_dim)
    angles = jnp.arange(length, dtype=jnp.float32)[:, None] * inverse[None, :]
    cosine = jnp.cos(angles)[:, None, :]
    sine_part = jnp.sin(angles)[:, None, :]
    lower_half = values[..., :half_dim]
    upper_half = values[..., half_dim:]
    return jnp.concatenate(
        [
            lower_half * cosine - upper_half * sine_part,
            upper_half * cosine + lower_half * sine_part,
        ],
        axis=-1,
    )


def carry_states(key_blocks, value_blocks, weighting, log_rates, block_size, backward):
    block_terms = jnp.einsum(
        "sbmhd,sbmhe->bshde",
        key_blocks * weighting[None, None, :, :, None],
        value_blocks,
        precision=highest_precision,
    )
    factor = jnp.exp(log_rates * block_size)[None, :, None, None]

    def advance(running, addend):
        return (running * factor + addend, running)

    initial = jnp.zeros(block_terms.shape[1:], jnp.float32)
    return lax.scan(advance, initial, block_terms, reverse=backward)[1]


def retain_blocks(
    query_rows, key_rows, value_rows, gate_rows, forward_decay, backward_decay, seq_count, length
):
    head_count = forward_decay.shape[0]
    head_dim = query_rows.shape[1] // head_count
    block_size = BLOCK
    block_count = length // block_size

    def split_heads(rows_in):
        return rows_in.astype(jnp.float32).reshape(seq_count, length, head_count, head_dim)

    def blocked(tensor):
        return tensor.reshape(seq_count, block_count, block_size, head_count, head_dim)

    queries = blocked(apply_rotary_heads(split_heads(query_rows), length))
    key_heads = blocked(apply_rotary_heads(split_heads(key_rows), length) * head_dim ** (-0.5))
    valued = blocked(split_heads(value_rows))
    rate_ahead = jax.nn.log_sigmoid(forward_decay)
    rate_behind = jax.nn.log_sigmoid(backward_decay)
    position = jnp.arange(block_size, dtype=jnp.float32)
    offset = position[:, None] - position[None, :]
    inside = jnp.where(
        offset[None] >= 0,
        jnp.exp(rate_ahead[:, None, None] * jnp.maximum(offset, 0.0)[None]),
        jnp.exp(rate_behind[:, None, None] * jnp.maximum(-offset, 0.0)[None]),
    )
    attention_scores = (
        jnp.einsum("sbchd,sbmhd->sbhcm", queries, key_heads, precision=highest_precision)
        * inside[None, None]
    )
    result = jnp.einsum("sbhcm,sbmhd->sbchd", attention_scores, valued, precision=highest_precision)
    column = position[:, None]
    key_ahead = jnp.exp(rate_ahead[None, :] * (block_size - 1 - column))
    query_ahead = jnp.exp(rate_ahead[None, :] * (column + 1))
    key_behind = jnp.exp(rate_behind[None, :] * column)
    query_behind = jnp.exp(rate_behind[None, :] * (block_size - column))
    from_before = carry_states(key_heads, valued, key_ahead, rate_ahead, block_size, False)
    from_after = carry_states(key_heads, valued, key_behind, rate_behind, block_size, True)
    result = (
        result
        + jnp.einsum("sbchd,bshde->sbche", queries, from_before, precision=highest_precision)
        * query_ahead[None, None, :, :, None]
    )
    result = (
        result
        + jnp.einsum("sbchd,bshde->sbche", queries, from_after, precision=highest_precision)
        * query_behind[None, None, :, :, None]
    )
    result = result.reshape(seq_count, length, head_count, head_dim)
    center = jnp.mean(result, axis=-1, keepdims=True)
    spread = jnp.mean(jnp.square(result - center), axis=-1, keepdims=True)
    normalized = (result - center) * lax.rsqrt(spread + group_eps)
    gated = jax.nn.silu(split_heads(gate_rows)) * normalized
    return gated.reshape(seq_count * length, head_count * head_dim).astype(jnp.bfloat16)


def on_device(
    tokens,
    input_gain,
    query_weight,
    key_weight,
    value_weight,
    output_gate_matrix,
    forward_decay,
    backward_decay,
    merge_weight,
    middle_gain,
    gate_weight,
    up_weight,
    down_weight,
):
    seq_count, length, part_width = tokens.shape
    row_count = seq_count * length
    pieces = (
        query_weight,
        key_weight,
        value_weight,
        output_gate_matrix,
        merge_weight.T,
        gate_weight,
        up_weight,
        down_weight.T,
    )
    packed = lax.all_gather(jnp.concatenate(pieces, axis=1), "fs", axis=0, tiled=True)
    full, at = [], 0
    for piece in pieces:
        full.append(packed[:, at : at + piece.shape[1]])
        at += piece.shape[1]
    query_full, key_full, value_full, gating_full, merge_full, gate_full, up_full, down_full = full

    local = tokens.reshape(row_count, part_width)
    normed = rms_scale(gathered_features(local), input_gain)

    def project(weight):
        return jnp.dot(normed, weight, preferred_element_type=jnp.float32).astype(jnp.bfloat16)

    mixed = retain_blocks(
        project(query_full),
        project(key_full),
        project(value_full),
        project(gating_full),
        forward_decay,
        backward_decay,
        seq_count,
        length,
    )
    merge_term = jnp.einsum("rh,dh->rd", mixed, merge_full, preferred_element_type=jnp.float32)
    merged = scattered_sum(merge_term.astype(jnp.bfloat16))
    middle = (local.astype(jnp.float32) + merged).astype(jnp.bfloat16)
    normed_mid = rms_scale(gathered_features(middle), middle_gain)
    gate_act = jnp.dot(normed_mid, gate_full, preferred_element_type=jnp.float32)
    up_act = jnp.dot(normed_mid, up_full, preferred_element_type=jnp.float32)
    hidden = (jax.nn.silu(gate_act) * up_act).astype(jnp.bfloat16)
    down_term = jnp.einsum("rh,dh->rd", hidden, down_full, preferred_element_type=jnp.float32)
    summed = scattered_sum(down_term.astype(jnp.bfloat16))
    layer_out = (middle.astype(jnp.float32) + summed).astype(jnp.bfloat16)
    return layer_out.reshape(seq_count, length, part_width)


def solution(mesh):
    placed = (
        P(("grp", "fs"), None, "tp"),
        P(),
        P("fs", "tp"),
        P("fs", "tp"),
        P("fs", "tp"),
        P("fs", "tp"),
        P("tp"),
        P("tp"),
        P("tp", "fs"),
        P(),
        P("fs", "tp"),
        P("fs", "tp"),
        P("tp", "fs"),
    )
    return jax.shard_map(
        on_device,
        mesh=mesh,
        in_specs=placed,
        out_specs=P(("grp", "fs"), None, "tp"),
        check_vma=False,
    )
```

```python
import jax
import jax.numpy as jnp
from jax import lax
from jax.sharding import PartitionSpec as P

BLOCK = 128


norm_eps = 1e-06
group_eps = 1e-05
rope_base = 10000.0
highest_precision = lax.Precision.HIGHEST


def core_pairs():
    peers = lax.axis_size("tp")
    return [[i, i + 1] for i in range(0, peers, 2)]


def chip_rings():
    peers = lax.axis_size("tp")
    return [list(range(0, peers, 2)), list(range(1, peers, 2))]


def gathered_features(shard):
    chips = lax.all_gather(shard, "tp", axis=0, axis_index_groups=chip_rings())
    both = jnp.broadcast_to(chips, (2, *chips.shape))
    both = lax.all_to_all(both, "tp", 0, 0, tiled=True, axis_index_groups=core_pairs())
    return jnp.concatenate(
        [both[c, x] for x in range(chips.shape[0]) for c in range(2)], axis=1
    )


def scattered_sum(partial_term):
    peers = lax.axis_size("tp")
    rows, width = partial_term.shape[0], partial_term.shape[1] // peers
    parts = [partial_term[:, t * width : (t + 1) * width] for t in range(peers)]
    tiles = jnp.stack([jnp.stack(parts[0::2]), jnp.stack(parts[1::2])])
    tiles = lax.all_to_all(tiles, "tp", 0, 0, tiled=True, axis_index_groups=core_pairs())
    chip_sum = (tiles[0].astype(jnp.float32) + tiles[1].astype(jnp.float32)).astype(jnp.bfloat16)
    tiles = lax.all_to_all(chip_sum, "tp", 0, 0, tiled=True, axis_index_groups=chip_rings())
    return jnp.sum(tiles.astype(jnp.float32), axis=0)


def group_pairs():
    return [(i, i ^ 1) for i in range(lax.axis_size("grp"))]


def parity_rings():
    peers = lax.axis_size("fs")
    return [list(range(0, peers, 2)), list(range(1, peers, 2))]


def from_neighbours(ring):
    peers = lax.axis_size("fs")
    half = ring.shape[0] // 2
    upper = lax.ppermute(ring[:half], "fs", [(i, (i - 1) % peers) for i in range(peers)])
    lower = lax.ppermute(ring[half:], "fs", [(i, (i + 1) % peers) for i in range(peers)])
    return jnp.concatenate([upper, lower], axis=0)


def in_order(own, other, block):
    first = lax.axis_index("fs") % 2 == 0
    own = own.reshape(-1, block, own.shape[1])
    other = other.reshape(own.shape)
    both = jnp.stack([jnp.where(first, own, other), jnp.where(first, other, own)], axis=1)
    return both.reshape(-1, own.shape[2])


def gathered_by_pairs(left, right, common):
    paired = lax.axis_size("grp") % 2 == 0
    block, width = left.shape
    if not paired:
        rows = []
        for piece in (left, right, common):
            ring = lax.all_gather(piece, "fs", axis=0, tiled=True, axis_index_groups=parity_rings())
            rows.append(in_order(ring, from_neighbours(ring), block))
        return rows
    lower = lax.axis_index("grp") % 2 == 0
    mine = jnp.concatenate([jnp.where(lower, left, right), common], axis=1)
    ring = lax.all_gather(mine, "fs", axis=0, tiled=True, axis_index_groups=parity_rings())
    near = from_neighbours(ring)
    ring_pair = lax.ppermute(ring[:, :width], "grp", group_pairs())
    near_pair = lax.ppermute(near[:, :width], "grp", group_pairs())
    mine = in_order(ring, near, block)
    theirs = in_order(ring_pair, near_pair, block)
    return mine[:, :width], theirs, mine[:, width:]


def rms_scale(values, gain_vector):
    widened = values.astype(jnp.float32)
    scaled = widened * lax.rsqrt(jnp.mean(widened * widened, axis=-1, keepdims=True) + norm_eps)
    return (scaled * gain_vector).astype(jnp.bfloat16)


def apply_rotary_heads(values, length):
    half_dim = values.shape[-1] // 2
    inverse = rope_base ** (-jnp.arange(half_dim, dtype=jnp.float32) / half_dim)
    angles = jnp.arange(length, dtype=jnp.float32)[:, None] * inverse[None, :]
    cosine = jnp.cos(angles)[:, None, :]
    sine_part = jnp.sin(angles)[:, None, :]
    lower_half = values[..., :half_dim]
    upper_half = values[..., half_dim:]
    return jnp.concatenate(
        [
            lower_half * cosine - upper_half * sine_part,
            upper_half * cosine + lower_half * sine_part,
        ],
        axis=-1,
    )


def carry_states(key_blocks, value_blocks, weighting, log_rates, block_size, backward):
    block_terms = jnp.einsum(
        "sbmhd,sbmhe->bshde",
        key_blocks * weighting[None, None, :, :, None],
        value_blocks,
        precision=highest_precision,
    )
    factor = jnp.exp(log_rates * block_size)[None, :, None, None]

    def advance(running, addend):
        return (running * factor + addend, running)

    initial = jnp.zeros(block_terms.shape[1:], jnp.float32)
    return lax.scan(advance, initial, block_terms, reverse=backward)[1]


def retain_blocks(
    query_rows, key_rows, value_rows, gate_rows, forward_decay, backward_decay, seq_count, length
):
    head_count = forward_decay.shape[0]
    head_dim = query_rows.shape[1] // head_count
    block_size = BLOCK
    block_count = length // block_size

    def split_heads(rows_in):
        return rows_in.astype(jnp.float32).reshape(seq_count, length, head_count, head_dim)

    def blocked(tensor):
        return tensor.reshape(seq_count, block_count, block_size, head_count, head_dim)

    queries = blocked(apply_rotary_heads(split_heads(query_rows), length))
    key_heads = blocked(apply_rotary_heads(split_heads(key_rows), length) * head_dim ** (-0.5))
    valued = blocked(split_heads(value_rows))
    rate_ahead = jax.nn.log_sigmoid(forward_decay)
    rate_behind = jax.nn.log_sigmoid(backward_decay)
    position = jnp.arange(block_size, dtype=jnp.float32)
    offset = position[:, None] - position[None, :]
    inside = jnp.where(
        offset[None] >= 0,
        jnp.exp(rate_ahead[:, None, None] * jnp.maximum(offset, 0.0)[None]),
        jnp.exp(rate_behind[:, None, None] * jnp.maximum(-offset, 0.0)[None]),
    )
    attention_scores = (
        jnp.einsum("sbchd,sbmhd->sbhcm", queries, key_heads, precision=highest_precision)
        * inside[None, None]
    )
    result = jnp.einsum("sbhcm,sbmhd->sbchd", attention_scores, valued, precision=highest_precision)
    column = position[:, None]
    key_ahead = jnp.exp(rate_ahead[None, :] * (block_size - 1 - column))
    query_ahead = jnp.exp(rate_ahead[None, :] * (column + 1))
    key_behind = jnp.exp(rate_behind[None, :] * column)
    query_behind = jnp.exp(rate_behind[None, :] * (block_size - column))
    from_before = carry_states(key_heads, valued, key_ahead, rate_ahead, block_size, False)
    from_after = carry_states(key_heads, valued, key_behind, rate_behind, block_size, True)
    result = (
        result
        + jnp.einsum("sbchd,bshde->sbche", queries, from_before, precision=highest_precision)
        * query_ahead[None, None, :, :, None]
    )
    result = (
        result
        + jnp.einsum("sbchd,bshde->sbche", queries, from_after, precision=highest_precision)
        * query_behind[None, None, :, :, None]
    )
    result = result.reshape(seq_count, length, head_count, head_dim)
    center = jnp.mean(result, axis=-1, keepdims=True)
    spread = jnp.mean(jnp.square(result - center), axis=-1, keepdims=True)
    normalized = (result - center) * lax.rsqrt(spread + group_eps)
    gated = jax.nn.silu(split_heads(gate_rows)) * normalized
    return gated.reshape(seq_count * length, head_count * head_dim).astype(jnp.bfloat16)


def on_device(
    tokens,
    input_gain,
    query_weight,
    key_weight,
    value_weight,
    output_gate_matrix,
    forward_decay,
    backward_decay,
    merge_weight,
    middle_gain,
    gate_weight,
    up_weight,
    down_weight,
):
    seq_count, length, part_width = tokens.shape
    row_count = seq_count * length
    packed = jnp.concatenate([gate_weight, up_weight, down_weight.T], axis=1)
    hidden_width = gate_weight.shape[1]
    packed = lax.all_gather(packed, "fs", axis=0, tiled=True)

    mine_full, theirs_full, merge_full = gathered_by_pairs(
        jnp.concatenate([query_weight, key_weight], axis=1),
        jnp.concatenate([value_weight, output_gate_matrix], axis=1),
        merge_weight.T,
    )
    local = tokens.reshape(row_count, part_width)
    normed = rms_scale(gathered_features(local), input_gain)

    def project(weight):
        return jnp.dot(normed, weight, preferred_element_type=jnp.float32).astype(jnp.bfloat16)

    mine_rows, theirs_rows = project(mine_full), project(theirs_full)
    lower = lax.axis_index("grp") % 2 == 0
    lower = jnp.logical_or(lower, lax.axis_size("grp") % 2 == 1)
    left_rows = jnp.where(lower, mine_rows, theirs_rows)
    right_rows = jnp.where(lower, theirs_rows, mine_rows)
    head_width = query_weight.shape[1]
    mixed = retain_blocks(
        left_rows[:, :head_width],
        left_rows[:, head_width:],
        right_rows[:, :head_width],
        right_rows[:, head_width:],
        forward_decay,
        backward_decay,
        seq_count,
        length,
    )
    merge_term = jnp.einsum("rh,dh->rd", mixed, merge_full, preferred_element_type=jnp.float32)
    merged = scattered_sum(merge_term.astype(jnp.bfloat16))
    middle = (local.astype(jnp.float32) + merged).astype(jnp.bfloat16)
    normed_mid = rms_scale(gathered_features(middle), middle_gain)
    gate_act = jnp.dot(normed_mid, packed[:, :hidden_width], preferred_element_type=jnp.float32)
    up_act = jnp.dot(normed_mid, packed[:, hidden_width : 2 * hidden_width], preferred_element_type=jnp.float32)
    hidden = (jax.nn.silu(gate_act) * up_act).astype(jnp.bfloat16)
    down_term = jnp.einsum("rh,dh->rd", hidden, packed[:, 2 * hidden_width :], preferred_element_type=jnp.float32)
    summed = scattered_sum(down_term.astype(jnp.bfloat16))
    layer_out = (middle.astype(jnp.float32) + summed).astype(jnp.bfloat16)
    return layer_out.reshape(seq_count, length, part_width)


def solution(mesh):
    placed = (
        P(("grp", "fs"), None, "tp"),
        P(),
        P("fs", "tp"),
        P("fs", "tp"),
        P("fs", "tp"),
        P("fs", "tp"),
        P("tp"),
        P("tp"),
        P("tp", "fs"),
        P(),
        P("fs", "tp"),
        P("fs", "tp"),
        P("tp", "fs"),
    )
    return jax.shard_map(
        on_device,
        mesh=mesh,
        in_specs=placed,
        out_specs=P(("grp", "fs"), None, "tp"),
        check_vma=False,
    )
```

```python
import jax
import jax.numpy as jnp
from jax import lax
from jax.experimental import pallas as pl
from jax.experimental.pallas import tpu as pltpu
from jax.sharding import PartitionSpec as P

BLOCK = 128


norm_eps = 1e-06
group_eps = 1e-05
rope_base = 10000.0
highest_precision = lax.Precision.HIGHEST


def core_pairs():
    peers = lax.axis_size("tp")
    return [[i, i + 1] for i in range(0, peers, 2)]


def chip_rings():
    peers = lax.axis_size("tp")
    return [list(range(0, peers, 2)), list(range(1, peers, 2))]


def gathered_features(shard):
    chips = lax.all_gather(shard, "tp", axis=0, axis_index_groups=chip_rings())
    both = jnp.broadcast_to(chips, (2, *chips.shape))
    both = lax.all_to_all(both, "tp", 0, 0, tiled=True, axis_index_groups=core_pairs())
    return jnp.concatenate(
        [both[c, x] for x in range(chips.shape[0]) for c in range(2)], axis=1
    )


def by_core_and_chip(partial_term):
    peers = lax.axis_size("tp")
    width = partial_term.shape[1] // peers
    parts = [partial_term[:, t * width : (t + 1) * width] for t in range(peers)]
    return jnp.stack([jnp.stack(parts[0::2]), jnp.stack(parts[1::2])])


def scattered_sum(tiles):
    tiles = lax.all_to_all(tiles, "tp", 0, 0, tiled=True, axis_index_groups=core_pairs())
    chip_sum = (tiles[0].astype(jnp.float32) + tiles[1].astype(jnp.float32)).astype(jnp.bfloat16)
    tiles = lax.all_to_all(chip_sum, "tp", 0, 0, tiled=True, axis_index_groups=chip_rings())
    return jnp.sum(tiles.astype(jnp.float32), axis=0)


def parity_rings():
    peers = lax.axis_size("fs")
    return [list(range(0, peers, 2)), list(range(1, peers, 2))]


def from_neighbours(ring):
    peers = lax.axis_size("fs")
    half = ring.shape[0] // 2
    upper = lax.ppermute(ring[:half], "fs", [(i, (i - 1) % peers) for i in range(peers)])
    lower = lax.ppermute(ring[half:], "fs", [(i, (i + 1) % peers) for i in range(peers)])
    return jnp.concatenate([upper, lower], axis=0)


def in_order(own, other, block):
    first = lax.axis_index("fs") % 2 == 0
    own = own.reshape(-1, block, own.shape[1])
    other = other.reshape(own.shape)
    both = jnp.stack([jnp.where(first, own, other), jnp.where(first, other, own)], axis=1)
    return both.reshape(-1, own.shape[2])


def gathered_rows(piece):
    scale = 2.0**17
    piece = (piece.astype(jnp.float32) * scale).astype(jnp.float16)
    ring = lax.all_gather(piece, "fs", axis=0, tiled=True, axis_index_groups=parity_rings())
    rows = in_order(ring, from_neighbours(ring), piece.shape[0])
    return (rows.astype(jnp.float32) * (1.0 / scale)).astype(jnp.bfloat16)


def rms_scale(values, gain_vector):
    widened = values.astype(jnp.float32)
    scaled = widened * lax.rsqrt(jnp.mean(widened * widened, axis=-1, keepdims=True) + norm_eps)
    return (scaled * gain_vector).astype(jnp.bfloat16)


def apply_rotary_heads(values, length):
    half_dim = values.shape[-1] // 2
    inverse = rope_base ** (-jnp.arange(half_dim, dtype=jnp.float32) / half_dim)
    angles = jnp.arange(length, dtype=jnp.float32)[:, None] * inverse[None, :]
    cosine = jnp.cos(angles)[:, None, :]
    sine_part = jnp.sin(angles)[:, None, :]
    lower_half = values[..., :half_dim]
    upper_half = values[..., half_dim:]
    return jnp.concatenate(
        [
            lower_half * cosine - upper_half * sine_part,
            upper_half * cosine + lower_half * sine_part,
        ],
        axis=-1,
    )


def carry_states(key_blocks, value_blocks, weighting, log_rates, block_size, backward):
    block_terms = jnp.einsum(
        "sbmhd,sbmhe->bshde",
        key_blocks * weighting[None, None, :, :, None],
        value_blocks,
        precision=highest_precision,
    )
    factor = jnp.exp(log_rates * block_size)[None, :, None, None]

    def advance(running, addend):
        return (running * factor + addend, running)

    initial = jnp.zeros(block_terms.shape[1:], jnp.float32)
    return lax.scan(advance, initial, block_terms, reverse=backward)[1]


def retain_blocks(
    query_rows, key_rows, value_rows, gate_rows, forward_decay, backward_decay, seq_count, length
):
    head_count = forward_decay.shape[0]
    head_dim = query_rows.shape[1] // head_count
    block_size = BLOCK
    block_count = length // block_size

    def split_heads(rows_in):
        return rows_in.astype(jnp.float32).reshape(seq_count, length, head_count, head_dim)

    def blocked(tensor):
        return tensor.reshape(seq_count, block_count, block_size, head_count, head_dim)

    queries = blocked(apply_rotary_heads(split_heads(query_rows), length))
    key_heads = blocked(apply_rotary_heads(split_heads(key_rows), length) * head_dim ** (-0.5))
    valued = blocked(split_heads(value_rows))
    rate_ahead = jax.nn.log_sigmoid(forward_decay)
    rate_behind = jax.nn.log_sigmoid(backward_decay)
    position = jnp.arange(block_size, dtype=jnp.float32)
    offset = position[:, None] - position[None, :]
    inside = jnp.where(
        offset[None] >= 0,
        jnp.exp(rate_ahead[:, None, None] * jnp.maximum(offset, 0.0)[None]),
        jnp.exp(rate_behind[:, None, None] * jnp.maximum(-offset, 0.0)[None]),
    )
    attention_scores = (
        jnp.einsum("sbchd,sbmhd->sbhcm", queries, key_heads, precision=highest_precision)
        * inside[None, None]
    )
    result = jnp.einsum("sbhcm,sbmhd->sbchd", attention_scores, valued, precision=highest_precision)
    column = position[:, None]
    key_ahead = jnp.exp(rate_ahead[None, :] * (block_size - 1 - column))
    query_ahead = jnp.exp(rate_ahead[None, :] * (column + 1))
    key_behind = jnp.exp(rate_behind[None, :] * column)
    query_behind = jnp.exp(rate_behind[None, :] * (block_size - column))
    from_before = carry_states(key_heads, valued, key_ahead, rate_ahead, block_size, False)
    from_after = carry_states(key_heads, valued, key_behind, rate_behind, block_size, True)
    result = (
        result
        + jnp.einsum("sbchd,bshde->sbche", queries, from_before, precision=highest_precision)
        * query_ahead[None, None, :, :, None]
    )
    result = (
        result
        + jnp.einsum("sbchd,bshde->sbche", queries, from_after, precision=highest_precision)
        * query_behind[None, None, :, :, None]
    )
    result = result.reshape(seq_count, length, head_count, head_dim)
    center = jnp.mean(result, axis=-1, keepdims=True)
    spread = jnp.mean(jnp.square(result - center), axis=-1, keepdims=True)
    normalized = (result - center) * lax.rsqrt(spread + group_eps)
    gated = jax.nn.silu(split_heads(gate_rows)) * normalized
    return gated.reshape(seq_count * length, head_count * head_dim).astype(jnp.bfloat16)


def feed_forward_kernel(
    normed_ref, packed_ref, out_ref, pair_ref, down_ref, hidden_ref, pair_sem, down_sem
):
    units = hidden_ref.shape[1]
    lanes = pair_ref.shape[2] // 2
    blocks, width = down_ref.shape[0], down_ref.shape[1]
    copies = []
    for j in range(units // lanes):
        for half in range(2):
            source = packed_ref.at[:, pl.ds(half * units + j * lanes, lanes)]
            target = pair_ref.at[j, :, pl.ds(half * lanes, lanes)]
            copies.append(pltpu.make_async_copy(source, target, pair_sem.at[j, half]))
    down_copies = []
    for t in range(blocks):
        source = packed_ref.at[pl.ds(t * width, width), pl.ds(2 * units, units)]
        down_copies.append(pltpu.make_async_copy(source, down_ref.at[t], down_sem.at[t]))
    for copy in copies + down_copies:
        copy.start()
    for j in range(units // lanes):
        copies[2 * j].wait()
        copies[2 * j + 1].wait()
        both = jnp.dot(normed_ref[...], pair_ref[j], preferred_element_type=jnp.float32)
        gate_act, up_act = both[:, :lanes], both[:, lanes:]
        hidden = gate_act / (1.0 + jnp.exp(-gate_act)) * up_act
        hidden_ref[:, j * lanes : (j + 1) * lanes] = hidden.astype(hidden_ref.dtype)
    for t in range(blocks):
        down_copies[t].wait()
        term = lax.dot_general(
            hidden_ref[...],
            down_ref[t],
            (((1,), (1,)), ((), ())),
            preferred_element_type=jnp.float32,
        )
        out_ref[t % 2, t // 2] = term.astype(out_ref.dtype)


def feed_forward(normed_mid, packed, peers):
    rows, features = normed_mid.shape
    units = packed.shape[1] // 3
    lanes, width = 128, features // peers
    return pl.pallas_call(
        feed_forward_kernel,
        out_shape=jax.ShapeDtypeStruct((2, peers // 2, rows, width), jnp.bfloat16),
        in_specs=[
            pl.BlockSpec(memory_space=pltpu.VMEM),
            pl.BlockSpec(memory_space=pltpu.HBM),
        ],
        out_specs=pl.BlockSpec(memory_space=pltpu.VMEM),
        scratch_shapes=[
            pltpu.VMEM((units // lanes, features, 2 * lanes), jnp.bfloat16),
            pltpu.VMEM((peers, width, units), jnp.bfloat16),
            pltpu.VMEM((rows, units), jnp.bfloat16),
            pltpu.SemaphoreType.DMA((units // lanes, 2)),
            pltpu.SemaphoreType.DMA((peers,)),
        ],
        compiler_params=pltpu.CompilerParams(vmem_limit_bytes=57 * 1024 * 1024),
    )(normed_mid, packed)


def on_device(
    tokens,
    input_gain,
    query_weight,
    key_weight,
    value_weight,
    output_gate_matrix,
    forward_decay,
    backward_decay,
    merge_weight,
    middle_gain,
    gate_weight,
    up_weight,
    down_weight,
):
    seq_count, length, part_width = tokens.shape
    row_count = seq_count * length
    packed = jnp.concatenate([gate_weight, up_weight, down_weight.T], axis=1)
    packed = lax.all_gather(packed, "fs", axis=0, tiled=True)

    first = gathered_rows(
        jnp.concatenate(
            [query_weight, key_weight, value_weight, output_gate_matrix, merge_weight.T], axis=1
        )
    )
    head_width = query_weight.shape[1]
    local = tokens.reshape(row_count, part_width)
    normed = rms_scale(gathered_features(local), input_gain)
    projected = jnp.dot(normed, first[:, : 4 * head_width], preferred_element_type=jnp.float32)
    projected = projected.astype(jnp.bfloat16)
    merge_full = first[:, 4 * head_width :]
    mixed = retain_blocks(
        projected[:, :head_width],
        projected[:, head_width : 2 * head_width],
        projected[:, 2 * head_width : 3 * head_width],
        projected[:, 3 * head_width :],
        forward_decay,
        backward_decay,
        seq_count,
        length,
    )
    merge_term = jnp.einsum("rh,dh->rd", mixed, merge_full, preferred_element_type=jnp.float32)
    merged = scattered_sum(by_core_and_chip(merge_term.astype(jnp.bfloat16)))
    middle = (local.astype(jnp.float32) + merged).astype(jnp.bfloat16)
    normed_mid = rms_scale(gathered_features(middle), middle_gain)
    summed = scattered_sum(feed_forward(normed_mid, packed, lax.axis_size("tp")))
    layer_out = (middle.astype(jnp.float32) + summed).astype(jnp.bfloat16)
    return layer_out.reshape(seq_count, length, part_width)


def solution(mesh):
    placed = (
        P(("grp", "fs"), None, "tp"),
        P(),
        P("fs", "tp"),
        P("fs", "tp"),
        P("fs", "tp"),
        P("fs", "tp"),
        P("tp"),
        P("tp"),
        P("tp", "fs"),
        P(),
        P("fs", "tp"),
        P("fs", "tp"),
        P("tp", "fs"),
    )
    return jax.shard_map(
        on_device,
        mesh=mesh,
        in_specs=placed,
        out_specs=P(("grp", "fs"), None, "tp"),
        check_vma=False,
    )
```

```python
import jax
import jax.numpy as jnp
from jax import lax
from jax.experimental import pallas as pl
from jax.experimental.pallas import tpu as pltpu
from jax.sharding import PartitionSpec as P


BLOCK = 128


norm_eps = 1e-06
group_eps = 1e-05
rope_base = 10000.0
highest_precision = lax.Precision.HIGHEST


def core_pairs():
    peers = lax.axis_size("tp")
    return [[i, i + 1] for i in range(0, peers, 2)]


def chip_rings():
    peers = lax.axis_size("tp")
    return [list(range(0, peers, 2)), list(range(1, peers, 2))]


def gathered_features(shard):
    chips = lax.all_gather(shard, "tp", axis=0, axis_index_groups=chip_rings())
    both = jnp.broadcast_to(chips, (2, *chips.shape))
    both = lax.all_to_all(both, "tp", 0, 0, tiled=True, axis_index_groups=core_pairs())
    return jnp.concatenate(
        [both[c, x] for x in range(chips.shape[0]) for c in range(2)], axis=1
    )


def by_core_and_chip(partial_term):
    peers = lax.axis_size("tp")
    width = partial_term.shape[1] // peers
    parts = [partial_term[:, t * width : (t + 1) * width] for t in range(peers)]
    return jnp.stack([jnp.stack(parts[0::2]), jnp.stack(parts[1::2])])


def scattered_sum(tiles):
    tiles = lax.all_to_all(tiles, "tp", 0, 0, tiled=True, axis_index_groups=core_pairs())
    chip_sum = (tiles[0].astype(jnp.float32) + tiles[1].astype(jnp.float32)).astype(jnp.bfloat16)
    tiles = lax.all_to_all(chip_sum, "tp", 0, 0, tiled=True, axis_index_groups=chip_rings())
    return jnp.sum(tiles.astype(jnp.float32), axis=0)


def group_pairs():
    return [(i, i ^ 1) for i in range(lax.axis_size("grp"))]


def parity_rings():
    peers = lax.axis_size("fs")
    return [list(range(0, peers, 2)), list(range(1, peers, 2))]


def from_neighbours(ring):
    peers = lax.axis_size("fs")
    half = ring.shape[0] // 2
    upper = lax.ppermute(ring[:half], "fs", [(i, (i - 1) % peers) for i in range(peers)])
    lower = lax.ppermute(ring[half:], "fs", [(i, (i + 1) % peers) for i in range(peers)])
    return jnp.concatenate([upper, lower], axis=0)


def in_order(own, other, block):
    first = lax.axis_index("fs") % 2 == 0
    own = own.reshape(-1, block, own.shape[1])
    other = other.reshape(own.shape)
    both = jnp.stack([jnp.where(first, own, other), jnp.where(first, other, own)], axis=1)
    return both.reshape(-1, own.shape[2])


def gathered_by_pairs(left, right, common):
    paired = lax.axis_size("grp") % 2 == 0
    block, width = left.shape
    if not paired:
        rows = []
        for piece in (left, right, common):
            ring = lax.all_gather(piece, "fs", axis=0, tiled=True, axis_index_groups=parity_rings())
            rows.append(in_order(ring, from_neighbours(ring), block))
        return rows
    lower = lax.axis_index("grp") % 2 == 0
    mine = jnp.concatenate([jnp.where(lower, left, right), common], axis=1)
    ring = lax.all_gather(mine, "fs", axis=0, tiled=True, axis_index_groups=parity_rings())
    near = from_neighbours(ring)
    ring_pair = lax.ppermute(ring[:, :width], "grp", group_pairs())
    near_pair = lax.ppermute(near[:, :width], "grp", group_pairs())
    mine = in_order(ring, near, block)
    theirs = in_order(ring_pair, near_pair, block)
    return mine[:, :width], theirs, mine[:, width:]


def rms_scale(values, gain_vector):
    widened = values.astype(jnp.float32)
    scaled = widened * lax.rsqrt(jnp.mean(widened * widened, axis=-1, keepdims=True) + norm_eps)
    return (scaled * gain_vector).astype(jnp.bfloat16)


def apply_rotary_heads(values, length):
    half_dim = values.shape[-1] // 2
    inverse = rope_base ** (-jnp.arange(half_dim, dtype=jnp.float32) / half_dim)
    angles = jnp.arange(length, dtype=jnp.float32)[:, None] * inverse[None, :]
    cosine = jnp.cos(angles)[:, None, :]
    sine_part = jnp.sin(angles)[:, None, :]
    lower_half = values[..., :half_dim]
    upper_half = values[..., half_dim:]
    return jnp.concatenate(
        [
            lower_half * cosine - upper_half * sine_part,
            upper_half * cosine + lower_half * sine_part,
        ],
        axis=-1,
    )


def carry_states(key_blocks, value_blocks, weighting, log_rates, block_size, backward):
    block_terms = jnp.einsum(
        "sbmhd,sbmhe->bshde",
        key_blocks * weighting[None, None, :, :, None],
        value_blocks,
        precision=highest_precision,
    )
    factor = jnp.exp(log_rates * block_size)[None, :, None, None]

    def advance(running, addend):
        return (running * factor + addend, running)

    initial = jnp.zeros(block_terms.shape[1:], jnp.float32)
    return lax.scan(advance, initial, block_terms, reverse=backward)[1]


def retain_blocks(
    query_rows, key_rows, value_rows, gate_rows, forward_decay, backward_decay, seq_count, length
):
    head_count = forward_decay.shape[0]
    head_dim = query_rows.shape[1] // head_count
    block_size = BLOCK
    block_count = length // block_size

    def split_heads(rows_in):
        return rows_in.astype(jnp.float32).reshape(seq_count, length, head_count, head_dim)

    def blocked(tensor):
        return tensor.reshape(seq_count, block_count, block_size, head_count, head_dim)

    queries = blocked(apply_rotary_heads(split_heads(query_rows), length))
    key_heads = blocked(apply_rotary_heads(split_heads(key_rows), length) * head_dim ** (-0.5))
    valued = blocked(split_heads(value_rows))
    rate_ahead = jax.nn.log_sigmoid(forward_decay)
    rate_behind = jax.nn.log_sigmoid(backward_decay)
    position = jnp.arange(block_size, dtype=jnp.float32)
    offset = position[:, None] - position[None, :]
    inside = jnp.where(
        offset[None] >= 0,
        jnp.exp(rate_ahead[:, None, None] * jnp.maximum(offset, 0.0)[None]),
        jnp.exp(rate_behind[:, None, None] * jnp.maximum(-offset, 0.0)[None]),
    )
    attention_scores = (
        jnp.einsum("sbchd,sbmhd->sbhcm", queries, key_heads, precision=highest_precision)
        * inside[None, None]
    )
    result = jnp.einsum("sbhcm,sbmhd->sbchd", attention_scores, valued, precision=highest_precision)
    column = position[:, None]
    key_ahead = jnp.exp(rate_ahead[None, :] * (block_size - 1 - column))
    query_ahead = jnp.exp(rate_ahead[None, :] * (column + 1))
    key_behind = jnp.exp(rate_behind[None, :] * column)
    query_behind = jnp.exp(rate_behind[None, :] * (block_size - column))
    from_before = carry_states(key_heads, valued, key_ahead, rate_ahead, block_size, False)
    from_after = carry_states(key_heads, valued, key_behind, rate_behind, block_size, True)
    result = (
        result
        + jnp.einsum("sbchd,bshde->sbche", queries, from_before, precision=highest_precision)
        * query_ahead[None, None, :, :, None]
    )
    result = (
        result
        + jnp.einsum("sbchd,bshde->sbche", queries, from_after, precision=highest_precision)
        * query_behind[None, None, :, :, None]
    )
    result = result.reshape(seq_count, length, head_count, head_dim)
    center = jnp.mean(result, axis=-1, keepdims=True)
    spread = jnp.mean(jnp.square(result - center), axis=-1, keepdims=True)
    normalized = (result - center) * lax.rsqrt(spread + group_eps)
    gated = jax.nn.silu(split_heads(gate_rows)) * normalized
    return gated.reshape(seq_count * length, head_count * head_dim).astype(jnp.bfloat16)


def feed_forward_kernel(
    normed_ref, packed_ref, out_ref, upper_ref, down_ref, acts_ref, upper_sem, down_sem
):
    units = down_ref.shape[1]
    blocks, depth = upper_ref.shape[0], upper_ref.shape[1]
    width = out_ref.shape[2]
    peers = out_ref.shape[0] * out_ref.shape[1]
    upper, down = [], []
    for k in range(blocks):
        rows = pl.ds(k * depth, depth)
        source = packed_ref.at[rows, pl.ds(0, 2 * units)]
        upper.append(pltpu.make_async_copy(source, upper_ref.at[k], upper_sem.at[k]))
    for k in range(blocks):
        rows = pl.ds(k * depth, depth)
        source = packed_ref.at[rows, pl.ds(2 * units, units)]
        down.append(pltpu.make_async_copy(source, down_ref.at[rows], down_sem.at[k]))
    for copy in upper + down:
        copy.start()
    for k in range(blocks):
        upper[k].wait()
        term = jnp.dot(
            normed_ref[:, k * depth : (k + 1) * depth],
            upper_ref[k],
            preferred_element_type=jnp.float32,
        )
        if k == 0:
            acts_ref[...] = term
        else:
            acts_ref[...] += term
    gate_act, up_act = acts_ref[:, :units], acts_ref[:, units:]
    hidden = gate_act / (1.0 + jnp.exp(-gate_act)) * up_act
    hidden = hidden.T.astype(jnp.bfloat16)
    for k in range(blocks):
        down[k].wait()
    for t in range(peers):
        term = jnp.dot(
            down_ref[t * width : (t + 1) * width], hidden, preferred_element_type=jnp.float32
        )
        out_ref[t % 2, t // 2] = term.astype(out_ref.dtype)


def feed_forward(normed_mid, packed, peers):
    rows, features = normed_mid.shape
    units = packed.shape[1] // 3
    width, depth = features // peers, 512
    blocks = features // depth
    return pl.pallas_call(
        feed_forward_kernel,
        out_shape=jax.ShapeDtypeStruct((2, peers // 2, width, rows), jnp.bfloat16),
        in_specs=[
            pl.BlockSpec(memory_space=pltpu.VMEM),
            pl.BlockSpec(memory_space=pltpu.HBM),
        ],
        out_specs=pl.BlockSpec(memory_space=pltpu.VMEM),
        scratch_shapes=[
            pltpu.VMEM((blocks, depth, 2 * units), jnp.bfloat16),
            pltpu.VMEM((features, units), jnp.bfloat16),
            pltpu.VMEM((rows, 2 * units), jnp.float32),
            pltpu.SemaphoreType.DMA((blocks,)),
            pltpu.SemaphoreType.DMA((blocks,)),
        ],
        compiler_params=pltpu.CompilerParams(vmem_limit_bytes=57 * 1024 * 1024),
    )(normed_mid, packed)


def on_device(
    tokens,
    input_gain,
    query_weight,
    key_weight,
    value_weight,
    output_gate_matrix,
    forward_decay,
    backward_decay,
    merge_weight,
    middle_gain,
    gate_weight,
    up_weight,
    down_weight,
):
    seq_count, length, part_width = tokens.shape
    row_count = seq_count * length
    packed = jnp.concatenate([gate_weight, up_weight, down_weight.T], axis=1)
    packed = lax.all_gather(packed, "fs", axis=0, tiled=True)

    mine_full, theirs_full, merge_full = gathered_by_pairs(
        jnp.concatenate([query_weight, key_weight], axis=1),
        jnp.concatenate([value_weight, output_gate_matrix], axis=1),
        merge_weight.T,
    )
    local = tokens.reshape(row_count, part_width)
    gathered = gathered_features(local)
    normed = rms_scale(gathered, input_gain)

    def project(weight):
        return jnp.dot(normed, weight, preferred_element_type=jnp.float32).astype(jnp.bfloat16)

    mine_rows, theirs_rows = project(mine_full), project(theirs_full)
    lower = lax.axis_index("grp") % 2 == 0
    lower = jnp.logical_or(lower, lax.axis_size("grp") % 2 == 1)
    left_rows = jnp.where(lower, mine_rows, theirs_rows)
    right_rows = jnp.where(lower, theirs_rows, mine_rows)
    head_width = query_weight.shape[1]
    mixed = retain_blocks(
        left_rows[:, :head_width],
        left_rows[:, head_width:],
        right_rows[:, :head_width],
        right_rows[:, head_width:],
        forward_decay,
        backward_decay,
        seq_count,
        length,
    )
    merge_term = jnp.einsum("rh,dh->rd", mixed, merge_full, preferred_element_type=jnp.float32)
    merged = scattered_sum(by_core_and_chip(merge_term.astype(jnp.bfloat16)))
    middle = (local.astype(jnp.float32) + merged).astype(jnp.bfloat16)
    normed_mid = rms_scale(gathered_features(middle), middle_gain)
    summed = scattered_sum(feed_forward(normed_mid, packed, lax.axis_size("tp"))).T
    layer_out = (middle.astype(jnp.float32) + summed).astype(jnp.bfloat16)
    return layer_out.reshape(seq_count, length, part_width)


def solution(mesh):
    placed = (
        P(("grp", "fs"), None, "tp"),
        P(),
        P("fs", "tp"),
        P("fs", "tp"),
        P("fs", "tp"),
        P("fs", "tp"),
        P("tp"),
        P("tp"),
        P("tp", "fs"),
        P(),
        P("fs", "tp"),
        P("fs", "tp"),
        P("tp", "fs"),
    )

    return jax.shard_map(
        on_device,
        mesh=mesh,
        in_specs=placed,
        out_specs=P(("grp", "fs"), None, "tp"),
        check_vma=False,
    )
```

```python
import jax
import jax.numpy as jnp
from jax import lax
from jax.experimental import pallas as pl
from jax.experimental.pallas import tpu as pltpu
from jax.sharding import PartitionSpec as P


BLOCK = 128


norm_eps = 1e-06
group_eps = 1e-05
rope_base = 10000.0
highest_precision = lax.Precision.HIGHEST


def core_pairs():
    peers = lax.axis_size("tp")
    return [[i, i + 1] for i in range(0, peers, 2)]


def chip_rings():
    peers = lax.axis_size("tp")
    return [list(range(0, peers, 2)), list(range(1, peers, 2))]


def gathered_features(shard):
    chips = lax.all_gather(shard, "tp", axis=0, axis_index_groups=chip_rings())
    both = jnp.broadcast_to(chips, (2, *chips.shape))
    both = lax.all_to_all(both, "tp", 0, 0, tiled=True, axis_index_groups=core_pairs())
    return jnp.concatenate(
        [both[c, x] for x in range(chips.shape[0]) for c in range(2)], axis=1
    )


def by_core_and_chip(partial_term):
    peers = lax.axis_size("tp")
    width = partial_term.shape[1] // peers
    parts = [partial_term[:, t * width : (t + 1) * width] for t in range(peers)]
    return jnp.stack([jnp.stack(parts[0::2]), jnp.stack(parts[1::2])])


def scattered_sum(tiles):
    tiles = lax.all_to_all(tiles, "tp", 0, 0, tiled=True, axis_index_groups=core_pairs())
    chip_sum = (tiles[0].astype(jnp.float32) + tiles[1].astype(jnp.float32)).astype(jnp.bfloat16)
    tiles = lax.all_to_all(chip_sum, "tp", 0, 0, tiled=True, axis_index_groups=chip_rings())
    return jnp.sum(tiles.astype(jnp.float32), axis=0)


def group_pairs():
    return [(i, i ^ 1) for i in range(lax.axis_size("grp"))]


def parity_rings():
    peers = lax.axis_size("fs")
    return [list(range(0, peers, 2)), list(range(1, peers, 2))]


def from_neighbours(ring):
    peers = lax.axis_size("fs")
    half = ring.shape[0] // 2
    upper = lax.ppermute(ring[:half], "fs", [(i, (i - 1) % peers) for i in range(peers)])
    lower = lax.ppermute(ring[half:], "fs", [(i, (i + 1) % peers) for i in range(peers)])
    return jnp.concatenate([upper, lower], axis=0)


def in_order(own, other, block):
    first = lax.axis_index("fs") % 2 == 0
    own = own.reshape(-1, block, own.shape[1])
    other = other.reshape(own.shape)
    both = jnp.stack([jnp.where(first, own, other), jnp.where(first, other, own)], axis=1)
    return both.reshape(-1, own.shape[2])


def gathered_by_pairs(left, right, common):
    paired = lax.axis_size("grp") % 2 == 0
    block, width = left.shape
    if not paired:
        rows = []
        for piece in (left, right, common):
            ring = lax.all_gather(piece, "fs", axis=0, tiled=True, axis_index_groups=parity_rings())
            rows.append(in_order(ring, from_neighbours(ring), block))
        return rows
    lower = lax.axis_index("grp") % 2 == 0
    mine = jnp.concatenate([jnp.where(lower, left, right), common], axis=1)
    ring = lax.all_gather(mine, "fs", axis=0, tiled=True, axis_index_groups=parity_rings())
    ring_pair = lax.ppermute(ring[:, :width], "grp", group_pairs())
    near = from_neighbours(ring)
    near_pair = from_neighbours(ring_pair)
    mine = in_order(ring, near, block)
    theirs = in_order(ring_pair, near_pair, block)
    return mine[:, :width], theirs, mine[:, width:]


def rms_scale(values, gain_vector):
    widened = values.astype(jnp.float32)
    scaled = widened * lax.rsqrt(jnp.mean(widened * widened, axis=-1, keepdims=True) + norm_eps)
    return (scaled * gain_vector).astype(jnp.bfloat16)


def apply_rotary_heads(values, length):
    half_dim = values.shape[-1] // 2
    inverse = rope_base ** (-jnp.arange(half_dim, dtype=jnp.float32) / half_dim)
    angles = jnp.arange(length, dtype=jnp.float32)[:, None] * inverse[None, :]
    cosine = jnp.cos(angles)[:, None, :]
    sine_part = jnp.sin(angles)[:, None, :]
    lower_half = values[..., :half_dim]
    upper_half = values[..., half_dim:]
    return jnp.concatenate(
        [
            lower_half * cosine - upper_half * sine_part,
            upper_half * cosine + lower_half * sine_part,
        ],
        axis=-1,
    )


def carry_states(key_blocks, value_blocks, weighting, log_rates, block_size, backward):
    block_terms = jnp.einsum(
        "sbmhd,sbmhe->bshde",
        key_blocks * weighting[None, None, :, :, None],
        value_blocks,
        precision=highest_precision,
    )
    factor = jnp.exp(log_rates * block_size)[None, :, None, None]

    def advance(running, addend):
        return (running * factor + addend, running)

    initial = jnp.zeros(block_terms.shape[1:], jnp.float32)
    return lax.scan(advance, initial, block_terms, reverse=backward)[1]


def retain_blocks(
    query_rows, key_rows, value_rows, gate_rows, forward_decay, backward_decay, seq_count, length
):
    head_count = forward_decay.shape[0]
    head_dim = query_rows.shape[1] // head_count
    block_size = BLOCK
    block_count = length // block_size

    def split_heads(rows_in):
        return rows_in.astype(jnp.float32).reshape(seq_count, length, head_count, head_dim)

    def blocked(tensor):
        return tensor.reshape(seq_count, block_count, block_size, head_count, head_dim)

    queries = blocked(apply_rotary_heads(split_heads(query_rows), length))
    key_heads = blocked(apply_rotary_heads(split_heads(key_rows), length) * head_dim ** (-0.5))
    valued = blocked(split_heads(value_rows))
    rate_ahead = jax.nn.log_sigmoid(forward_decay)
    rate_behind = jax.nn.log_sigmoid(backward_decay)
    position = jnp.arange(block_size, dtype=jnp.float32)
    offset = position[:, None] - position[None, :]
    inside = jnp.where(
        offset[None] >= 0,
        jnp.exp(rate_ahead[:, None, None] * jnp.maximum(offset, 0.0)[None]),
        jnp.exp(rate_behind[:, None, None] * jnp.maximum(-offset, 0.0)[None]),
    )
    attention_scores = (
        jnp.einsum("sbchd,sbmhd->sbhcm", queries, key_heads, precision=highest_precision)
        * inside[None, None]
    )
    result = jnp.einsum("sbhcm,sbmhd->sbchd", attention_scores, valued, precision=highest_precision)
    column = position[:, None]
    key_ahead = jnp.exp(rate_ahead[None, :] * (block_size - 1 - column))
    query_ahead = jnp.exp(rate_ahead[None, :] * (column + 1))
    key_behind = jnp.exp(rate_behind[None, :] * column)
    query_behind = jnp.exp(rate_behind[None, :] * (block_size - column))
    from_before = carry_states(key_heads, valued, key_ahead, rate_ahead, block_size, False)
    from_after = carry_states(key_heads, valued, key_behind, rate_behind, block_size, True)
    result = (
        result
        + jnp.einsum("sbchd,bshde->sbche", queries, from_before, precision=highest_precision)
        * query_ahead[None, None, :, :, None]
    )
    result = (
        result
        + jnp.einsum("sbchd,bshde->sbche", queries, from_after, precision=highest_precision)
        * query_behind[None, None, :, :, None]
    )
    result = result.reshape(seq_count, length, head_count, head_dim)
    center = jnp.mean(result, axis=-1, keepdims=True)
    spread = jnp.mean(jnp.square(result - center), axis=-1, keepdims=True)
    normalized = (result - center) * lax.rsqrt(spread + group_eps)
    gated = jax.nn.silu(split_heads(gate_rows)) * normalized
    return gated.reshape(seq_count * length, head_count * head_dim).astype(jnp.bfloat16)


def feed_forward_kernel(
    normed_ref, packed_ref, out_ref, upper_ref, down_ref, acts_ref, upper_sem, down_sem
):
    units = down_ref.shape[1]
    blocks, depth = upper_ref.shape[0], upper_ref.shape[1]
    width = out_ref.shape[3]
    peers = out_ref.shape[0] * out_ref.shape[1]
    upper, down = [], []
    for k in range(blocks):
        rows = pl.ds(k * depth, depth)
        source = packed_ref.at[rows, pl.ds(0, 2 * units)]
        upper.append(pltpu.make_async_copy(source, upper_ref.at[k], upper_sem.at[k]))
    for k in range(blocks):
        rows = pl.ds(k * depth, depth)
        source = packed_ref.at[rows, pl.ds(2 * units, units)]
        down.append(pltpu.make_async_copy(source, down_ref.at[rows], down_sem.at[k]))
    for copy in upper + down:
        copy.start()
    for k in range(blocks):
        upper[k].wait()
        term = jnp.dot(
            normed_ref[:, k * depth : (k + 1) * depth],
            upper_ref[k],
            preferred_element_type=jnp.float32,
        )
        if k == 0:
            acts_ref[...] = term
        else:
            acts_ref[...] += term
    gate_act, up_act = acts_ref[:, :units], acts_ref[:, units:]
    hidden = (gate_act / (1.0 + jnp.exp(-gate_act)) * up_act).astype(jnp.bfloat16)
    for k in range(blocks):
        down[k].wait()
    for t in range(peers):
        term = lax.dot_general(
            hidden,
            down_ref[t * width : (t + 1) * width],
            (((1,), (1,)), ((), ())),
            preferred_element_type=jnp.float32,
        )
        out_ref[t % 2, t // 2] = term.astype(out_ref.dtype)


def feed_forward(normed_mid, packed, peers):
    rows, features = normed_mid.shape
    units = packed.shape[1] // 3
    width, depth = features // peers, 512
    blocks = features // depth
    return pl.pallas_call(
        feed_forward_kernel,
        out_shape=jax.ShapeDtypeStruct((2, peers // 2, rows, width), jnp.bfloat16),
        in_specs=[
            pl.BlockSpec(memory_space=pltpu.VMEM),
            pl.BlockSpec(memory_space=pltpu.HBM),
        ],
        out_specs=pl.BlockSpec(memory_space=pltpu.VMEM),
        scratch_shapes=[
            pltpu.VMEM((blocks, depth, 2 * units), jnp.bfloat16),
            pltpu.VMEM((features, units), jnp.bfloat16),
            pltpu.VMEM((rows, 2 * units), jnp.float32),
            pltpu.SemaphoreType.DMA((blocks,)),
            pltpu.SemaphoreType.DMA((blocks,)),
        ],
        compiler_params=pltpu.CompilerParams(vmem_limit_bytes=57 * 1024 * 1024),
    )(normed_mid, packed)


def on_device(
    tokens,
    input_gain,
    query_weight,
    key_weight,
    value_weight,
    output_gate_matrix,
    forward_decay,
    backward_decay,
    merge_weight,
    middle_gain,
    gate_weight,
    up_weight,
    down_weight,
):
    seq_count, length, part_width = tokens.shape
    row_count = seq_count * length
    packed = jnp.concatenate([gate_weight, up_weight, down_weight.T], axis=1)
    packed = lax.all_gather(packed, "fs", axis=0, tiled=True)

    mine_full, theirs_full, merge_full = gathered_by_pairs(
        jnp.concatenate([query_weight, key_weight], axis=1),
        jnp.concatenate([value_weight, output_gate_matrix], axis=1),
        merge_weight.T,
    )
    local = tokens.reshape(row_count, part_width)
    normed = rms_scale(gathered_features(local), input_gain)

    def project(weight):
        return jnp.dot(normed, weight, preferred_element_type=jnp.float32).astype(jnp.bfloat16)

    mine_rows, theirs_rows = project(mine_full), project(theirs_full)
    lower = lax.axis_index("grp") % 2 == 0
    lower = jnp.logical_or(lower, lax.axis_size("grp") % 2 == 1)
    left_rows = jnp.where(lower, mine_rows, theirs_rows)
    right_rows = jnp.where(lower, theirs_rows, mine_rows)
    head_width = query_weight.shape[1]
    mixed = retain_blocks(
        left_rows[:, :head_width],
        left_rows[:, head_width:],
        right_rows[:, :head_width],
        right_rows[:, head_width:],
        forward_decay,
        backward_decay,
        seq_count,
        length,
    )
    merge_term = jnp.einsum("rh,dh->rd", mixed, merge_full, preferred_element_type=jnp.float32)
    merged = scattered_sum(by_core_and_chip(merge_term.astype(jnp.bfloat16)))
    middle = (local.astype(jnp.float32) + merged).astype(jnp.bfloat16)
    normed_mid = rms_scale(gathered_features(middle), middle_gain)
    summed = scattered_sum(feed_forward(normed_mid, packed, lax.axis_size("tp")))
    layer_out = (middle.astype(jnp.float32) + summed).astype(jnp.bfloat16)
    return layer_out.reshape(seq_count, length, part_width)


def solution(mesh):
    placed = (
        P(("grp", "fs"), None, "tp"),
        P(),
        P("fs", "tp"),
        P("fs", "tp"),
        P("fs", "tp"),
        P("fs", "tp"),
        P("tp"),
        P("tp"),
        P("tp", "fs"),
        P(),
        P("fs", "tp"),
        P("fs", "tp"),
        P("tp", "fs"),
    )

    return jax.shard_map(
        on_device,
        mesh=mesh,
        in_specs=placed,
        out_specs=P(("grp", "fs"), None, "tp"),
        check_vma=False,
    )
```

```python
import jax
import jax.numpy as jnp
from jax import lax
from jax.experimental import pallas as pl
from jax.experimental.pallas import tpu as pltpu
from jax.sharding import PartitionSpec as P


BLOCK = 128


norm_eps = 1e-06
group_eps = 1e-05
rope_base = 10000.0
highest_precision = lax.Precision.HIGHEST


def core_pairs():
    peers = lax.axis_size("tp")
    return [[i, i + 1] for i in range(0, peers, 2)]


def chip_rings():
    peers = lax.axis_size("tp")
    return [list(range(0, peers, 2)), list(range(1, peers, 2))]


def gathered_features(shard):
    chips = lax.all_gather(shard, "tp", axis=0, axis_index_groups=chip_rings())
    both = jnp.broadcast_to(chips, (2, *chips.shape))
    both = lax.all_to_all(both, "tp", 0, 0, tiled=True, axis_index_groups=core_pairs())
    return jnp.concatenate(
        [both[c, x] for x in range(chips.shape[0]) for c in range(2)], axis=1
    )


def by_core_and_chip(partial_term):
    peers = lax.axis_size("tp")
    width = partial_term.shape[1] // peers
    parts = [partial_term[:, t * width : (t + 1) * width] for t in range(peers)]
    return jnp.stack([jnp.stack(parts[0::2]), jnp.stack(parts[1::2])])


def scattered_sum(tiles):
    tiles = lax.all_to_all(tiles, "tp", 0, 0, tiled=True, axis_index_groups=core_pairs())
    return sum_over_chips(tiles[0], tiles[1])


def sum_over_chips(mine, theirs):
    chip_sum = (mine.astype(jnp.float32) + theirs.astype(jnp.float32)).astype(jnp.bfloat16)
    tiles = lax.all_to_all(chip_sum, "tp", 0, 0, tiled=True, axis_index_groups=chip_rings())
    return jnp.sum(tiles.astype(jnp.float32), axis=0)


def group_pairs():
    return [(i, i ^ 1) for i in range(lax.axis_size("grp"))]


def parity_rings():
    peers = lax.axis_size("fs")
    return [list(range(0, peers, 2)), list(range(1, peers, 2))]


def from_neighbours(ring):
    peers = lax.axis_size("fs")
    half = ring.shape[0] // 2
    upper = lax.ppermute(ring[:half], "fs", [(i, (i - 1) % peers) for i in range(peers)])
    lower = lax.ppermute(ring[half:], "fs", [(i, (i + 1) % peers) for i in range(peers)])
    return jnp.concatenate([upper, lower], axis=0)


def in_order(own, other, block):
    first = lax.axis_index("fs") % 2 == 0
    own = own.reshape(-1, block, own.shape[1])
    other = other.reshape(own.shape)
    both = jnp.stack([jnp.where(first, own, other), jnp.where(first, other, own)], axis=1)
    return both.reshape(-1, own.shape[2])


def gathered_by_pairs(left, right, common):
    paired = lax.axis_size("grp") % 2 == 0
    block, width = left.shape
    if not paired:
        rows = []
        for piece in (left, right, common):
            ring = lax.all_gather(piece, "fs", axis=0, tiled=True, axis_index_groups=parity_rings())
            rows.append(in_order(ring, from_neighbours(ring), block))
        return rows
    lower = lax.axis_index("grp") % 2 == 0
    mine = jnp.concatenate([jnp.where(lower, left, right), common], axis=1)
    ring = lax.all_gather(mine, "fs", axis=0, tiled=True, axis_index_groups=parity_rings())
    ring_pair = lax.ppermute(ring[:, :width], "grp", group_pairs())
    near = from_neighbours(ring)
    near_pair = from_neighbours(ring_pair)
    mine = in_order(ring, near, block)
    theirs = in_order(ring_pair, near_pair, block)
    return mine[:, :width], theirs, mine[:, width:]


def rms_scale(values, gain_vector):
    widened = values.astype(jnp.float32)
    scaled = widened * lax.rsqrt(jnp.mean(widened * widened, axis=-1, keepdims=True) + norm_eps)
    return (scaled * gain_vector).astype(jnp.bfloat16)


def apply_rotary_heads(values, length):
    half_dim = values.shape[-1] // 2
    inverse = rope_base ** (-jnp.arange(half_dim, dtype=jnp.float32) / half_dim)
    angles = jnp.arange(length, dtype=jnp.float32)[:, None] * inverse[None, :]
    cosine = jnp.cos(angles)[:, None, :]
    sine_part = jnp.sin(angles)[:, None, :]
    lower_half = values[..., :half_dim]
    upper_half = values[..., half_dim:]
    return jnp.concatenate(
        [
            lower_half * cosine - upper_half * sine_part,
            upper_half * cosine + lower_half * sine_part,
        ],
        axis=-1,
    )


def carry_states(key_blocks, value_blocks, weighting, log_rates, block_size, backward):
    block_terms = jnp.einsum(
        "sbmhd,sbmhe->bshde",
        key_blocks * weighting[None, None, :, :, None],
        value_blocks,
        precision=highest_precision,
    )
    factor = jnp.exp(log_rates * block_size)[None, :, None, None]

    def advance(running, addend):
        return (running * factor + addend, running)

    initial = jnp.zeros(block_terms.shape[1:], jnp.float32)
    return lax.scan(advance, initial, block_terms, reverse=backward)[1]


def retain_blocks(
    query_rows, key_rows, value_rows, gate_rows, forward_decay, backward_decay, seq_count, length
):
    head_count = forward_decay.shape[0]
    head_dim = query_rows.shape[1] // head_count
    block_size = BLOCK
    block_count = length // block_size

    def split_heads(rows_in):
        return rows_in.astype(jnp.float32).reshape(seq_count, length, head_count, head_dim)

    def blocked(tensor):
        return tensor.reshape(seq_count, block_count, block_size, head_count, head_dim)

    queries = blocked(apply_rotary_heads(split_heads(query_rows), length))
    key_heads = blocked(apply_rotary_heads(split_heads(key_rows), length) * head_dim ** (-0.5))
    valued = blocked(split_heads(value_rows))
    rate_ahead = jax.nn.log_sigmoid(forward_decay)
    rate_behind = jax.nn.log_sigmoid(backward_decay)
    position = jnp.arange(block_size, dtype=jnp.float32)
    offset = position[:, None] - position[None, :]
    inside = jnp.where(
        offset[None] >= 0,
        jnp.exp(rate_ahead[:, None, None] * jnp.maximum(offset, 0.0)[None]),
        jnp.exp(rate_behind[:, None, None] * jnp.maximum(-offset, 0.0)[None]),
    )
    attention_scores = (
        jnp.einsum("sbchd,sbmhd->sbhcm", queries, key_heads, precision=highest_precision)
        * inside[None, None]
    )
    result = jnp.einsum("sbhcm,sbmhd->sbchd", attention_scores, valued, precision=highest_precision)
    column = position[:, None]
    key_ahead = jnp.exp(rate_ahead[None, :] * (block_size - 1 - column))
    query_ahead = jnp.exp(rate_ahead[None, :] * (column + 1))
    key_behind = jnp.exp(rate_behind[None, :] * column)
    query_behind = jnp.exp(rate_behind[None, :] * (block_size - column))
    from_before = carry_states(key_heads, valued, key_ahead, rate_ahead, block_size, False)
    from_after = carry_states(key_heads, valued, key_behind, rate_behind, block_size, True)
    result = (
        result
        + jnp.einsum("sbchd,bshde->sbche", queries, from_before, precision=highest_precision)
        * query_ahead[None, None, :, :, None]
    )
    result = (
        result
        + jnp.einsum("sbchd,bshde->sbche", queries, from_after, precision=highest_precision)
        * query_behind[None, None, :, :, None]
    )
    result = result.reshape(seq_count, length, head_count, head_dim)
    center = jnp.mean(result, axis=-1, keepdims=True)
    spread = jnp.mean(jnp.square(result - center), axis=-1, keepdims=True)
    normalized = (result - center) * lax.rsqrt(spread + group_eps)
    gated = jax.nn.silu(split_heads(gate_rows)) * normalized
    return gated.reshape(seq_count * length, head_count * head_dim).astype(jnp.bfloat16)


def down_share(hidden_ref, weights):
    return lax.dot_general(
        hidden_ref[...], weights, (((1,), (1,)), ((), ())), preferred_element_type=jnp.float32
    ).astype(jnp.bfloat16)


def feed_forward_kernel(
    core_ref,
    normed_ref,
    packed_ref,
    other_ref,
    hidden_ref,
    own_down_ref,
    upper_ref,
    down_ref,
    acts_ref,
    upper_sem,
    down_sem,
    own_sem,
):
    units = hidden_ref.shape[1]
    blocks, depth = upper_ref.shape[0], upper_ref.shape[1]
    chips, width = down_ref.shape[0], down_ref.shape[1]
    core = core_ref[0]
    upper, down, own = [], [], []
    for k in range(blocks):
        source = packed_ref.at[pl.ds(k * depth, depth), pl.ds(0, 2 * units)]
        upper.append(pltpu.make_async_copy(source, upper_ref.at[k], upper_sem.at[k]))
    for chip in range(chips):
        rows = pl.ds((2 * chip + 1 - core) * width, width)
        source = packed_ref.at[rows, pl.ds(2 * units, units)]
        down.append(pltpu.make_async_copy(source, down_ref.at[chip], down_sem.at[chip]))
    for chip in range(chips):
        rows = pl.ds((2 * chip + core) * width, width)
        source = packed_ref.at[rows, pl.ds(2 * units, units)]
        own.append(pltpu.make_async_copy(source, own_down_ref.at[chip], own_sem.at[chip]))
    for copy in upper + down + own:
        copy.start()
    for k in range(blocks):
        upper[k].wait()
        term = jnp.dot(
            normed_ref[:, k * depth : (k + 1) * depth],
            upper_ref[k],
            preferred_element_type=jnp.float32,
        )
        if k == 0:
            acts_ref[...] = term
        else:
            acts_ref[...] += term
    gate_act, up_act = acts_ref[:, :units], acts_ref[:, units:]
    hidden = gate_act / (1.0 + jnp.exp(-gate_act)) * up_act
    hidden_ref[...] = hidden.astype(hidden_ref.dtype)
    for copy in down + own:
        copy.wait()
    for chip in range(chips):
        other_ref[chip] = down_share(hidden_ref, down_ref[chip])


def own_share_kernel(hidden_ref, own_down_ref, own_ref):
    for chip in range(own_ref.shape[0]):
        own_ref[chip] = down_share(hidden_ref, own_down_ref[chip])


def feed_forward(normed_mid, packed, core, peers):
    rows, features = normed_mid.shape
    units = packed.shape[1] // 3
    chips, width, depth = peers // 2, features // peers, 512
    blocks = features // depth
    vmem = pl.BlockSpec(memory_space=pltpu.VMEM)
    return pl.pallas_call(
        feed_forward_kernel,
        out_shape=[
            jax.ShapeDtypeStruct((chips, rows, width), jnp.bfloat16),
            jax.ShapeDtypeStruct((rows, units), jnp.bfloat16),
            jax.ShapeDtypeStruct((chips, width, units), jnp.bfloat16),
        ],
        in_specs=[
            pl.BlockSpec(memory_space=pltpu.SMEM),
            vmem,
            pl.BlockSpec(memory_space=pltpu.HBM),
        ],
        out_specs=[vmem, vmem, vmem],
        scratch_shapes=[
            pltpu.VMEM((blocks, depth, 2 * units), jnp.bfloat16),
            pltpu.VMEM((chips, width, units), jnp.bfloat16),
            pltpu.VMEM((rows, 2 * units), jnp.float32),
            pltpu.SemaphoreType.DMA((blocks,)),
            pltpu.SemaphoreType.DMA((chips,)),
            pltpu.SemaphoreType.DMA((chips,)),
        ],
        compiler_params=pltpu.CompilerParams(vmem_limit_bytes=48 * 1024 * 1024),
    )(core, normed_mid, packed)


def own_share(hidden, own_down):
    chips, width, _ = own_down.shape
    vmem = pl.BlockSpec(memory_space=pltpu.VMEM)
    return pl.pallas_call(
        own_share_kernel,
        out_shape=jax.ShapeDtypeStruct((chips, hidden.shape[0], width), jnp.bfloat16),
        in_specs=[vmem, vmem],
        out_specs=vmem,
        compiler_params=pltpu.CompilerParams(vmem_limit_bytes=8 * 1024 * 1024),
    )(hidden, own_down)


def on_device(
    tokens,
    input_gain,
    query_weight,
    key_weight,
    value_weight,
    output_gate_matrix,
    forward_decay,
    backward_decay,
    merge_weight,
    middle_gain,
    gate_weight,
    up_weight,
    down_weight,
):
    seq_count, length, part_width = tokens.shape
    row_count = seq_count * length
    packed = jnp.concatenate([gate_weight, up_weight, down_weight.T], axis=1)
    packed = lax.all_gather(packed, "fs", axis=0, tiled=True)

    mine_full, theirs_full, merge_full = gathered_by_pairs(
        jnp.concatenate([query_weight, key_weight], axis=1),
        jnp.concatenate([value_weight, output_gate_matrix], axis=1),
        merge_weight.T,
    )
    local = tokens.reshape(row_count, part_width)
    normed = rms_scale(gathered_features(local), input_gain)

    def project(weight):
        return jnp.dot(normed, weight, preferred_element_type=jnp.float32).astype(jnp.bfloat16)

    mine_rows, theirs_rows = project(mine_full), project(theirs_full)
    lower = lax.axis_index("grp") % 2 == 0
    lower = jnp.logical_or(lower, lax.axis_size("grp") % 2 == 1)
    left_rows = jnp.where(lower, mine_rows, theirs_rows)
    right_rows = jnp.where(lower, theirs_rows, mine_rows)
    head_width = query_weight.shape[1]
    mixed = retain_blocks(
        left_rows[:, :head_width],
        left_rows[:, head_width:],
        right_rows[:, :head_width],
        right_rows[:, head_width:],
        forward_decay,
        backward_decay,
        seq_count,
        length,
    )
    merge_term = jnp.einsum("rh,dh->rd", mixed, merge_full, preferred_element_type=jnp.float32)
    merged = scattered_sum(by_core_and_chip(merge_term.astype(jnp.bfloat16)))
    middle = (local.astype(jnp.float32) + merged).astype(jnp.bfloat16)
    normed_mid = rms_scale(gathered_features(middle), middle_gain)
    peers = lax.axis_size("tp")
    core = (lax.axis_index("tp") % 2).astype(jnp.int32).reshape(1)
    other, hidden, own_down = feed_forward(normed_mid, packed, core, peers)
    theirs = lax.ppermute(other, "tp", [(i, i ^ 1) for i in range(peers)])
    mine = own_share(hidden, own_down)
    summed = sum_over_chips(mine, theirs)
    layer_out = (middle.astype(jnp.float32) + summed).astype(jnp.bfloat16)
    return layer_out.reshape(seq_count, length, part_width)


def solution(mesh):
    placed = (
        P(("grp", "fs"), None, "tp"),
        P(),
        P("fs", "tp"),
        P("fs", "tp"),
        P("fs", "tp"),
        P("fs", "tp"),
        P("tp"),
        P("tp"),
        P("tp", "fs"),
        P(),
        P("fs", "tp"),
        P("fs", "tp"),
        P("tp", "fs"),
    )

    return jax.shard_map(
        on_device,
        mesh=mesh,
        in_specs=placed,
        out_specs=P(("grp", "fs"), None, "tp"),
        check_vma=False,
    )
```

```python
import jax
import jax.numpy as jnp
from jax import lax
from jax.experimental import pallas as pl
from jax.experimental.pallas import tpu as pltpu
from jax.sharding import PartitionSpec as P


BLOCK = 128


norm_eps = 1e-06
group_eps = 1e-05
rope_base = 10000.0
highest_precision = lax.Precision.HIGHEST


def core_pairs():
    peers = lax.axis_size("tp")
    return [[i, i + 1] for i in range(0, peers, 2)]


def chip_rings():
    peers = lax.axis_size("tp")
    return [list(range(0, peers, 2)), list(range(1, peers, 2))]


def gathered_features(shard):
    chips = lax.all_gather(shard, "tp", axis=0, axis_index_groups=chip_rings())
    both = jnp.broadcast_to(chips, (2, *chips.shape))
    both = lax.all_to_all(both, "tp", 0, 0, tiled=True, axis_index_groups=core_pairs())
    return jnp.concatenate(
        [both[c, x] for x in range(chips.shape[0]) for c in range(2)], axis=1
    )


def by_core_and_chip(partial_term):
    peers = lax.axis_size("tp")
    width = partial_term.shape[1] // peers
    parts = [partial_term[:, t * width : (t + 1) * width] for t in range(peers)]
    return jnp.stack([jnp.stack(parts[0::2]), jnp.stack(parts[1::2])])


def scattered_sum(tiles):
    tiles = lax.all_to_all(tiles, "tp", 0, 0, tiled=True, axis_index_groups=core_pairs())
    return sum_over_chips(tiles[0], tiles[1])


def sum_over_chips(mine, theirs):
    chip_sum = (mine.astype(jnp.float32) + theirs.astype(jnp.float32)).astype(jnp.bfloat16)
    tiles = lax.all_to_all(chip_sum, "tp", 0, 0, tiled=True, axis_index_groups=chip_rings())
    return jnp.sum(tiles.astype(jnp.float32), axis=0)


def group_pairs():
    return [(i, i ^ 1) for i in range(lax.axis_size("grp"))]


def parity_rings():
    peers = lax.axis_size("fs")
    return [list(range(0, peers, 2)), list(range(1, peers, 2))]


def from_neighbours(ring):
    peers = lax.axis_size("fs")
    half = ring.shape[0] // 2
    upper = lax.ppermute(ring[:half], "fs", [(i, (i - 1) % peers) for i in range(peers)])
    lower = lax.ppermute(ring[half:], "fs", [(i, (i + 1) % peers) for i in range(peers)])
    return jnp.concatenate([upper, lower], axis=0)


def in_order(own, other, block):
    first = lax.axis_index("fs") % 2 == 0
    own = own.reshape(-1, block, own.shape[1])
    other = other.reshape(own.shape)
    both = jnp.stack([jnp.where(first, own, other), jnp.where(first, other, own)], axis=1)
    return both.reshape(-1, own.shape[2])


def gathered_by_pairs(left, right, common):
    paired = lax.axis_size("grp") % 2 == 0
    block, width = left.shape
    if not paired:
        rows = []
        for piece in (left, right, common):
            ring = lax.all_gather(piece, "fs", axis=0, tiled=True, axis_index_groups=parity_rings())
            rows.append(in_order(ring, from_neighbours(ring), block))
        return rows
    lower = lax.axis_index("grp") % 2 == 0
    mine = jnp.concatenate([jnp.where(lower, left, right), common], axis=1)
    ring = lax.all_gather(mine, "fs", axis=0, tiled=True, axis_index_groups=parity_rings())
    ring_pair = lax.ppermute(ring[:, :width], "grp", group_pairs())
    near = from_neighbours(ring)
    near_pair = from_neighbours(ring_pair)
    mine = in_order(ring, near, block)
    theirs = in_order(ring_pair, near_pair, block)
    return mine[:, :width], theirs, mine[:, width:]


def rms_scale(values, gain_vector):
    widened = values.astype(jnp.float32)
    scaled = widened * lax.rsqrt(jnp.mean(widened * widened, axis=-1, keepdims=True) + norm_eps)
    return (scaled * gain_vector).astype(jnp.bfloat16)


def apply_rotary_heads(values, length):
    half_dim = values.shape[-1] // 2
    inverse = rope_base ** (-jnp.arange(half_dim, dtype=jnp.float32) / half_dim)
    angles = jnp.arange(length, dtype=jnp.float32)[:, None] * inverse[None, :]
    cosine = jnp.cos(angles)[:, None, :]
    sine_part = jnp.sin(angles)[:, None, :]
    lower_half = values[..., :half_dim]
    upper_half = values[..., half_dim:]
    return jnp.concatenate(
        [
            lower_half * cosine - upper_half * sine_part,
            upper_half * cosine + lower_half * sine_part,
        ],
        axis=-1,
    )


def carry_states(key_blocks, value_blocks, weighting, log_rates, block_size, backward):
    block_terms = jnp.einsum(
        "sbmhd,sbmhe->bshde",
        key_blocks * weighting[None, None, :, :, None],
        value_blocks,
        precision=highest_precision,
    )
    factor = jnp.exp(log_rates * block_size)[None, :, None, None]

    def advance(running, addend):
        return (running * factor + addend, running)

    initial = jnp.zeros(block_terms.shape[1:], jnp.float32)
    return lax.scan(advance, initial, block_terms, reverse=backward)[1]


def retain_blocks(
    query_rows, key_rows, value_rows, gate_rows, forward_decay, backward_decay, seq_count, length
):
    head_count = forward_decay.shape[0]
    head_dim = query_rows.shape[1] // head_count
    block_size = BLOCK
    block_count = length // block_size

    def split_heads(rows_in):
        return rows_in.astype(jnp.float32).reshape(seq_count, length, head_count, head_dim)

    def blocked(tensor):
        return tensor.reshape(seq_count, block_count, block_size, head_count, head_dim)

    queries = blocked(apply_rotary_heads(split_heads(query_rows), length))
    key_heads = blocked(apply_rotary_heads(split_heads(key_rows), length) * head_dim ** (-0.5))
    valued = blocked(split_heads(value_rows))
    rate_ahead = jax.nn.log_sigmoid(forward_decay)
    rate_behind = jax.nn.log_sigmoid(backward_decay)
    position = jnp.arange(block_size, dtype=jnp.float32)
    offset = position[:, None] - position[None, :]
    inside = jnp.where(
        offset[None] >= 0,
        jnp.exp(rate_ahead[:, None, None] * jnp.maximum(offset, 0.0)[None]),
        jnp.exp(rate_behind[:, None, None] * jnp.maximum(-offset, 0.0)[None]),
    )
    attention_scores = (
        jnp.einsum("sbchd,sbmhd->sbhcm", queries, key_heads, precision=highest_precision)
        * inside[None, None]
    )
    result = jnp.einsum("sbhcm,sbmhd->sbchd", attention_scores, valued, precision=highest_precision)
    column = position[:, None]
    key_ahead = jnp.exp(rate_ahead[None, :] * (block_size - 1 - column))
    query_ahead = jnp.exp(rate_ahead[None, :] * (column + 1))
    key_behind = jnp.exp(rate_behind[None, :] * column)
    query_behind = jnp.exp(rate_behind[None, :] * (block_size - column))
    from_before = carry_states(key_heads, valued, key_ahead, rate_ahead, block_size, False)
    from_after = carry_states(key_heads, valued, key_behind, rate_behind, block_size, True)
    result = (
        result
        + jnp.einsum("sbchd,bshde->sbche", queries, from_before, precision=highest_precision)
        * query_ahead[None, None, :, :, None]
    )
    result = (
        result
        + jnp.einsum("sbchd,bshde->sbche", queries, from_after, precision=highest_precision)
        * query_behind[None, None, :, :, None]
    )
    result = result.reshape(seq_count, length, head_count, head_dim)
    center = jnp.mean(result, axis=-1, keepdims=True)
    spread = jnp.mean(jnp.square(result - center), axis=-1, keepdims=True)
    normalized = (result - center) * lax.rsqrt(spread + group_eps)
    gated = jax.nn.silu(split_heads(gate_rows)) * normalized
    return gated.reshape(seq_count * length, head_count * head_dim).astype(jnp.bfloat16)


def down_share(hidden_ref, weights):
    return lax.dot_general(
        hidden_ref[...], weights, (((1,), (1,)), ((), ())), preferred_element_type=jnp.float32
    ).astype(jnp.bfloat16)


def feed_forward_kernel(
    core_ref,
    normed_ref,
    packed_ref,
    other_ref,
    hidden_ref,
    own_down_ref,
    upper_ref,
    down_ref,
    acts_ref,
    upper_sem,
    down_sem,
    own_sem,
):
    units = hidden_ref.shape[1]
    blocks, depth = upper_ref.shape[0], upper_ref.shape[1]
    chips, width = down_ref.shape[0], down_ref.shape[1]
    core, here = core_ref[0], core_ref[1]
    order = [lax.rem(here + ahead, chips) for ahead in range(chips)]
    upper, down, own = [], [], []
    for k in range(blocks):
        source = packed_ref.at[pl.ds(k * depth, depth), pl.ds(0, 2 * units)]
        upper.append(pltpu.make_async_copy(source, upper_ref.at[k], upper_sem.at[k]))
    for chip in range(chips):
        rows = pl.ds((2 * order[chip] + 1 - core) * width, width)
        source = packed_ref.at[rows, pl.ds(2 * units, units)]
        down.append(pltpu.make_async_copy(source, down_ref.at[chip], down_sem.at[chip]))
    for chip in range(chips):
        rows = pl.ds((2 * order[chip] + core) * width, width)
        source = packed_ref.at[rows, pl.ds(2 * units, units)]
        own.append(pltpu.make_async_copy(source, own_down_ref.at[chip], own_sem.at[chip]))
    for copy in upper + down + own:
        copy.start()
    for k in range(blocks):
        upper[k].wait()
        term = jnp.dot(
            normed_ref[:, k * depth : (k + 1) * depth],
            upper_ref[k],
            preferred_element_type=jnp.float32,
        )
        if k == 0:
            acts_ref[...] = term
        else:
            acts_ref[...] += term
    gate_act, up_act = acts_ref[:, :units], acts_ref[:, units:]
    hidden = gate_act / (1.0 + jnp.exp(-gate_act)) * up_act
    hidden_ref[...] = hidden.astype(hidden_ref.dtype)
    for copy in down + own:
        copy.wait()
    for chip in range(chips):
        other_ref[chip] = down_share(hidden_ref, down_ref[chip])


def own_share_kernel(hidden_ref, own_down_ref, own_ref):
    for chip in range(own_ref.shape[0]):
        own_ref[chip] = down_share(hidden_ref, own_down_ref[chip])


def feed_forward(normed_mid, packed, core, peers):
    rows, features = normed_mid.shape
    units = packed.shape[1] // 3
    chips, width, depth = peers // 2, features // peers, 512
    blocks = features // depth
    vmem = pl.BlockSpec(memory_space=pltpu.VMEM)
    return pl.pallas_call(
        feed_forward_kernel,
        out_shape=[
            jax.ShapeDtypeStruct((chips, rows, width), jnp.bfloat16),
            jax.ShapeDtypeStruct((rows, units), jnp.bfloat16),
            jax.ShapeDtypeStruct((chips, width, units), jnp.bfloat16),
        ],
        in_specs=[
            pl.BlockSpec(memory_space=pltpu.SMEM),
            vmem,
            pl.BlockSpec(memory_space=pltpu.HBM),
        ],
        out_specs=[vmem, vmem, vmem],
        scratch_shapes=[
            pltpu.VMEM((blocks, depth, 2 * units), jnp.bfloat16),
            pltpu.VMEM((chips, width, units), jnp.bfloat16),
            pltpu.VMEM((rows, 2 * units), jnp.float32),
            pltpu.SemaphoreType.DMA((blocks,)),
            pltpu.SemaphoreType.DMA((chips,)),
            pltpu.SemaphoreType.DMA((chips,)),
        ],
        compiler_params=pltpu.CompilerParams(vmem_limit_bytes=48 * 1024 * 1024),
    )(core, normed_mid, packed)


def own_share(hidden, own_down):
    chips, width, _ = own_down.shape
    vmem = pl.BlockSpec(memory_space=pltpu.VMEM)
    return pl.pallas_call(
        own_share_kernel,
        out_shape=jax.ShapeDtypeStruct((chips, hidden.shape[0], width), jnp.bfloat16),
        in_specs=[vmem, vmem],
        out_specs=vmem,
        compiler_params=pltpu.CompilerParams(vmem_limit_bytes=8 * 1024 * 1024),
    )(hidden, own_down)


def on_device(
    tokens,
    input_gain,
    query_weight,
    key_weight,
    value_weight,
    output_gate_matrix,
    forward_decay,
    backward_decay,
    merge_weight,
    middle_gain,
    gate_weight,
    up_weight,
    down_weight,
):
    seq_count, length, part_width = tokens.shape
    row_count = seq_count * length
    packed = jnp.concatenate([gate_weight, up_weight, down_weight.T], axis=1)
    packed = lax.all_gather(packed, "fs", axis=0, tiled=True)

    mine_full, theirs_full, merge_full = gathered_by_pairs(
        jnp.concatenate([query_weight, key_weight], axis=1),
        jnp.concatenate([value_weight, output_gate_matrix], axis=1),
        merge_weight.T,
    )
    local = tokens.reshape(row_count, part_width)
    normed = rms_scale(gathered_features(local), input_gain)

    def project(weight):
        return jnp.dot(normed, weight, preferred_element_type=jnp.float32).astype(jnp.bfloat16)

    mine_rows, theirs_rows = project(mine_full), project(theirs_full)
    lower = lax.axis_index("grp") % 2 == 0
    lower = jnp.logical_or(lower, lax.axis_size("grp") % 2 == 1)
    left_rows = jnp.where(lower, mine_rows, theirs_rows)
    right_rows = jnp.where(lower, theirs_rows, mine_rows)
    head_width = query_weight.shape[1]
    mixed = retain_blocks(
        left_rows[:, :head_width],
        left_rows[:, head_width:],
        right_rows[:, :head_width],
        right_rows[:, head_width:],
        forward_decay,
        backward_decay,
        seq_count,
        length,
    )
    merge_term = jnp.einsum("rh,dh->rd", mixed, merge_full, preferred_element_type=jnp.float32)
    merged = scattered_sum(by_core_and_chip(merge_term.astype(jnp.bfloat16)))
    middle = (local.astype(jnp.float32) + merged).astype(jnp.bfloat16)
    normed_mid = rms_scale(gathered_features(middle), middle_gain)
    peers = lax.axis_size("tp")
    place = lax.axis_index("tp").astype(jnp.int32)
    core = jnp.stack([place % 2, place // 2])
    other, hidden, own_down = feed_forward(normed_mid, packed, core, peers)
    theirs = lax.ppermute(other, "tp", [(i, i ^ 1) for i in range(peers)])
    mine = own_share(hidden, own_down)
    chip_sum = (mine.astype(jnp.float32) + theirs.astype(jnp.float32)).astype(jnp.bfloat16)
    summed = chip_sum[0].astype(jnp.float32)
    for ahead in (2, 1, 3):
        steps = [(i, (i + 2 * ahead) % peers) for i in range(peers)]
        arrived = lax.ppermute(chip_sum[ahead], "tp", steps)
        summed = summed + arrived.astype(jnp.float32)
    layer_out = (middle.astype(jnp.float32) + summed).astype(jnp.bfloat16)
    return layer_out.reshape(seq_count, length, part_width)


def solution(mesh):
    placed = (
        P(("grp", "fs"), None, "tp"),
        P(),
        P("fs", "tp"),
        P("fs", "tp"),
        P("fs", "tp"),
        P("fs", "tp"),
        P("tp"),
        P("tp"),
        P("tp", "fs"),
        P(),
        P("fs", "tp"),
        P("fs", "tp"),
        P("tp", "fs"),
    )

    return jax.shard_map(
        on_device,
        mesh=mesh,
        in_specs=placed,
        out_specs=P(("grp", "fs"), None, "tp"),
        check_vma=False,
    )
```
